128 devices in a mesh: sp: 16 (over z, x), fs: 4 (over y), tp: 2 (over core).
Axes of the slice: x: 4, y: 4, z: 4, core: 2. Of those that a mesh axis runs over, the one named last changes fastest.
Arguments:
- tokens: bfloat16 [32768, 2048], P(('fs', 'sp')), parts along dimension 0, may hold values from -6 to 6
- norm_gain: bfloat16 [2048], replicated, may hold values from 0.099609375 to 1.8984375
- w_query: bfloat16 [2048, 1024], P('sp', 'tp'), may hold values from -0.15625 to 0.15625
- w_key: bfloat16 [2048, 256], P('sp', 'tp'), may hold values from -0.15625 to 0.15625
- w_value: bfloat16 [2048, 256], P('sp', 'tp'), may hold values from -0.125 to 0.125
- w_glu_value: bfloat16 [2048, 1024], P('sp', 'tp'), may hold values from -0.22097087 to 0.22097087
- w_glu_gate: bfloat16 [2048, 1024], P('sp', 'tp'), may hold values from -0.125 to 0.125
- conv_taps: bfloat16 [31, 1024], P(None, 'tp'), may hold values from -1 to 1
- convolution_norm_gain: bfloat16 [1024], replicated, may hold values from 0.099609375 to 1.8984375
- head_gain: bfloat16 [128], replicated, may hold values from 0.099609375 to 1.8984375
- lam: float32 [8], P('tp'), may hold values from 0.3 to 0.8
- w_out: bfloat16 [2048, 2048], P(None, 'sp'), may hold values from -0.125 to 0.125
Outputs:
- mixed: bfloat16 [32768, 2048], P(('fs', 'sp', 'tp')), parts along dimension 0
- log_totals: float32 [32768, 16], P(('fs', 'sp'), 'tp'), parts along dimension 0
The draws below stay inside these ranges and needn't reach their ends.
There are 4 independent parts, one for each index of `fs`. The reference program is written for one: setup_inputs(seed, part) draws one part's arguments, and reference() takes and returns one part's arrays. A program takes and returns all parts, laid end to end along the dimension named above; an argument that names none is the same for every part. Nothing has to cross between parts.
All inputs are finite; a program needn't handle non-finite values.
Results may differ from the reference program's by a relative error of at most 0.0095.
Values may be sent and summed in bfloat16 or wider, within the bound.
A program may use at most 64 MiB of HBM per device.

```python
import math
import jax
import jax.numpy as jnp
from jax import lax

D = 2048
HEADS = 8
KV_HEADS = 2
QK = 64
VDIM = 128
CONV = 1024
KW = 31
SEQ = 8192


def draw_w_glu_value(key, part):
    first, second = jax.random.split(jax.random.fold_in(key, 41))
    placed = (jnp.arange(CONV, dtype=jnp.float32) + jax.random.uniform(first, (CONV,), jnp.float32)) / CONV
    column_scale = 10.0 ** placed / 4.0
    base = jax.random.truncated_normal(second, -4.0, 4.0, (D, CONV), jnp.float32)
    values = base * column_scale[None, :] * D ** (-0.5)
    return jnp.clip(values, -10.0 * D ** (-0.5), 10.0 * D ** (-0.5)).astype(jnp.bfloat16)


def block_scale(own_key, dims, cuts, low, high):
    def one(axis_at, shards_of):
        draws = jax.random.uniform(jax.random.fold_in(jax.random.fold_in(own_key, 6), axis_at), (shards_of,), jnp.float32, low / len(cuts), high / len(cuts))
        return jnp.repeat(jnp.exp(draws), dims[axis_at] // shards_of).reshape((-1,) + (1,) * (len(dims) - axis_at - 1))

    level = one(*cuts[0])
    for cut in cuts[1:]:
        level = level * one(*cut)
    return level


def bell_draw(key, extent, scale, limit, cuts=(), kind=jnp.bfloat16):
    entries = jax.random.normal(key, extent, jnp.float32) * scale
    if len(cuts) > 0:
        entries = block_scale(key, extent, cuts, -0.22, 0.18) * entries
    return jnp.clip(entries, min=-limit, max=limit).astype(kind)


def setup_inputs(seed: int = 0, part: int = 0) -> dict:
    streams_of = jax.random.split(jax.random.key(seed), 13)
    part_keys = jax.random.split(jax.random.fold_in(streams_of[12], part), 13)
    return {
        "tokens": bell_draw(part_keys[0], (SEQ, D), 1.0, 6.0, ((0, 16),)),
        "norm_gain": jnp.clip(1.0 + 0.18 * jax.random.normal(streams_of[1], (D,), jnp.float32), 0.099609375, 1.8984375).astype(jnp.bfloat16),
        "w_query": bell_draw(streams_of[2], (D, HEADS * 2 * QK), (D * 2 // 3) ** -0.5, 0.15625, ((0, 16), (1, 2))),
        "w_key": bell_draw(streams_of[3], (D, KV_HEADS * 2 * QK), (D * 2 // 3) ** -0.5, 0.15625, ((0, 16), (1, 2))),
        "w_value": bell_draw(streams_of[4], (D, KV_HEADS * VDIM), D ** -0.5, 0.125, ((0, 16), (1, 2))),
        "w_glu_value": draw_w_glu_value(jax.random.fold_in(streams_of[12], 71), part),
        "w_glu_gate": bell_draw(streams_of[6], (D, CONV), D ** -0.5, 0.125, ((0, 16), (1, 2))),
        "conv_taps": bell_draw(streams_of[7], (KW, CONV), KW ** -0.5, 1.0, ((1, 2),)),
        "convolution_norm_gain": jnp.clip(1.0 + 0.18 * jax.random.normal(streams_of[8], (CONV,), jnp.float32), 0.099609375, 1.8984375).astype(jnp.bfloat16),
        "head_gain": jnp.clip(1.0 + 0.18 * jax.random.normal(streams_of[9], (VDIM,), jnp.float32), 0.099609375, 1.8984375).astype(jnp.bfloat16),
        "lam": jnp.clip(0.3 + 0.5 * jax.random.uniform(streams_of[10], (HEADS,), jnp.float32) ** block_scale(streams_of[10], (HEADS,), ((0, 2),), -0.2, 0.2), 0.3, 0.8),
        "w_out": bell_draw(streams_of[11], (HEADS * VDIM + CONV, D), (HEADS * VDIM + CONV) ** -0.5, 0.125, ((1, 16),)),
    }


def reference(tokens, norm_gain, w_query, w_key, w_value, w_glu_value, w_glu_gate, conv_taps, convolution_norm_gain, head_gain, lam, w_out):
    length = tokens.shape[0]
    eps = 1e-06
    tok32 = tokens.astype(jnp.float32)
    normalized_rows = (tok32 * lax.rsqrt(lax.optimization_barrier(jnp.mean(tok32 * tok32, axis=-1, keepdims=True)) + eps) * norm_gain.astype(jnp.float32)).astype(jnp.bfloat16)
    queries = jnp.dot(normalized_rows, w_query, preferred_element_type=jnp.float32).astype(jnp.bfloat16)
    keys = jnp.dot(normalized_rows, w_key, preferred_element_type=jnp.float32).astype(jnp.bfloat16)
    values = jnp.dot(normalized_rows, w_value, preferred_element_type=jnp.float32).astype(jnp.bfloat16)
    glu_val = jnp.dot(normalized_rows, w_glu_value, preferred_element_type=jnp.float32)
    glu_gate = jnp.dot(normalized_rows, w_glu_gate, preferred_element_type=jnp.float32)
    gated = (glu_val * jax.nn.sigmoid(glu_gate)).astype(jnp.bfloat16)
    padded = jnp.concatenate([jnp.zeros((KW - 1, CONV), jnp.bfloat16), gated], axis=0)
    conv = jnp.zeros((length, CONV), jnp.float32)
    for tap in range(KW):
        conv = conv + conv_taps[tap].astype(jnp.float32) * padded[tap:tap + length].astype(jnp.float32)
    conv = conv.astype(jnp.bfloat16).astype(jnp.float32)
    conv_act = jax.nn.silu(conv * lax.rsqrt(lax.optimization_barrier(jnp.mean(conv * conv, axis=-1, keepdims=True)) + eps) * convolution_norm_gain.astype(jnp.float32)).astype(jnp.bfloat16)
    group = HEADS // KV_HEADS
    key_all = keys.astype(jnp.float32).reshape(length, KV_HEADS, 2, QK)
    value_rows_full = values.astype(jnp.float32).reshape(length, KV_HEADS, VDIM)
    block = math.gcd(length, 512)
    query_blocks = queries.reshape(length // block, block, KV_HEADS, group, 2, QK)
    key_pos = jnp.arange(length, dtype=jnp.int32)

    def one_block(item):
        query_block, index = item
        qfloat = query_block.astype(jnp.float32)
        score = jnp.einsum('tkgmd,nkmd->tkgmn', qfloat, key_all) * QK ** (-0.5)
        query_pos = index * block + jnp.arange(block, dtype=jnp.int32)
        allowed = key_pos[None, None, None, None, :] <= query_pos[:, None, None, None, None]
        weight = jnp.where(allowed, jnp.exp(score), 0.0)
        total = lax.optimization_barrier(jnp.sum(weight, axis=-1))
        rounded_values = weight.astype(jnp.bfloat16).astype(jnp.float32)
        running_total = jnp.einsum('doejz,zow->doejw', rounded_values, value_rows_full)
        return (running_total, total)
    running_total, total = lax.map(one_block, (query_blocks, jnp.arange(length // block, dtype=jnp.int32)))
    running_total = running_total.reshape(length, HEADS, 2, VDIM)
    total = total.reshape(length, HEADS, 2)
    lam32 = lam.astype(jnp.float32)
    diff = running_total[:, :, 0] / total[:, :, 0, None] - lam32[None, :, None] * running_total[:, :, 1] / total[:, :, 1, None]
    att_out = diff * lax.rsqrt(lax.optimization_barrier(jnp.mean(diff * diff, axis=-1, keepdims=True)) + eps) * head_gain.astype(jnp.float32)
    att_out = att_out.astype(jnp.bfloat16).reshape(length, HEADS * VDIM)
    log_totals = jnp.log(total).reshape(length, HEADS * 2)
    both = jnp.concatenate([att_out, conv_act], axis=1)
    mixed = jnp.dot(both, w_out, preferred_element_type=jnp.float32).astype(jnp.bfloat16)
    return (mixed, log_totals)
```

```python
import functools
import math

import jax
import jax.numpy as jnp
from jax import lax
from jax.experimental import pallas as pl
from jax.experimental.pallas import tpu as pltpu
from jax.sharding import PartitionSpec as P

HEADS = 8
QK = 64
VDIM = 128
CONV = 1024
EPS = 1e-06
RING = 16
ROUNDS = 8
MESH = pl.DeviceIdType.MESH
ANY = pl.BlockSpec(memory_space=pl.ANY)
F32 = jnp.float32
BF16 = jnp.bfloat16


def dot(a, b):
    return jnp.dot(a, b, preferred_element_type=F32)


def place_on(cycle, sp):
    z, x = lax.div(sp, 4), lax.rem(sp, 4)
    lead = z if cycle == 0 else x
    return lead * 4 + lax.rem(z + x, 4)


def member_at(cycle, place):
    place = lax.rem(place + 2 * RING, RING)
    lead = lax.div(place, 4)
    other = lax.rem(lax.rem(place, 4) - lead + 4, 4)
    return lead * 4 + other if cycle == 0 else other * 4 + lead


def kernel(
    tok_hbm, ngain_ref, wq_hbm, wk_hbm, wv_hbm, wgv_hbm, wgg_hbm, taps_ref, cgain_ref, hgain_ref, lam_ref, wout_hbm,
    mixed_ref, logt_ref,
    tok, normed, wa, wg, wo, kv, q, acc, lsum, gpad, conv, squares, both, outbox, inbox, rim_out, sq_in,
    load_sem, send_sem, recv_sem, side_send, side_recv, out_send, out_recv,
):
    rows = tok.shape[0]
    me = lax.axis_index("sp")
    core = lax.axis_index("tp")
    places = [place_on(c, me) for c in range(2)]
    ahead = [member_at(d // 2, places[d // 2] + (1 if d % 2 == 0 else 15)) for d in range(4)]
    after, before = lax.rem(me + 1, RING), lax.rem(me + RING - 1, RING)

    mine = pl.ds(pl.multiple_of(me * 128, 128), 128)
    att_rows = pl.ds(pl.multiple_of(core * 512, 512), 512)
    conv_rows = pl.ds(pl.multiple_of(1024 + core * 512, 512), 512)
    loads = [
        (wk_hbm, wa.at[mine, pl.ds(0, 128)]),
        (wv_hbm, wa.at[mine, pl.ds(128, 128)]),
        (wq_hbm, wa.at[mine, pl.ds(256, 512)]),
        (wgv_hbm, wg.at[mine, pl.ds(0, 512)]),
        (wgg_hbm, wg.at[mine, pl.ds(512, 512)]),
        (tok_hbm, tok),
        (wout_hbm.at[att_rows], wo.at[me, pl.ds(0, 512)]),
        (wout_hbm.at[conv_rows], wo.at[me, pl.ds(512, 512)]),
    ]
    loads = [pltpu.make_async_copy(s, d, load_sem.at[i]) for i, (s, d) in enumerate(loads)]
    for load in loads:
        load.start()

    barrier = pltpu.get_barrier_semaphore()
    for peer in ahead + [after, before]:
        pl.semaphore_signal(barrier, inc=1, device_id={"sp": peer}, device_id_type=MESH)
    pl.semaphore_signal(barrier, inc=1, device_id={"tp": 1 - core}, device_id_type=MESH)
    pl.semaphore_wait(barrier, 7)

    def weight_rows(ref):
        def part(source, cycle, at, size):
            start = source * 128 + cycle * 64 + at * 64 // 2
            return ref.at[pl.ds(pl.multiple_of(start, 32), size * 32)]
        return part

    def out_rows(source, cycle, at, size):
        return wo.at[source, pl.ds(cycle * 512 + at * 256, size * 256)]

    def kv_rows(source, cycle, at, size):
        return kv.at[source * 2 + cycle, pl.ds(at * 256, size * 256)]

    jobs = [weight_rows(wa), weight_rows(wg), kv_rows, out_rows]
    WA, WG, KV, WO = range(4)

    def copy_of(job, d, r, last):
        cycle, way = d // 2, d % 2
        sign = 1 if way == 0 else -1
        source = member_at(cycle, places[cycle] - sign * (r - 1))
        at, size = (way, 1) if last else (0, 2)
        ref = jobs[job](source, cycle, at, size)
        return pltpu.make_async_remote_copy(
            src_ref=ref, dst_ref=ref, send_sem=send_sem.at[job, d, r - 1], recv_sem=recv_sem.at[job, d, r - 1],
            device_id={"sp": ahead[d]}, device_id_type=MESH,
        )

    def arrival_of(job, d, r, last):
        cycle, way = d // 2, d % 2
        sign = 1 if way == 0 else -1
        source = member_at(cycle, places[cycle] - sign * r)
        at, size = (way, 1) if last else (0, 2)
        ref = jobs[job](source, cycle, at, size)
        return pltpu.make_async_remote_copy(
            src_ref=ref, dst_ref=ref, send_sem=send_sem.at[job, d, r - 1], recv_sem=recv_sem.at[job, d, r - 1],
            device_id={"sp": ahead[d]}, device_id_type=MESH,
        )

    def send(job, r, last=False):
        for d in range(4):
            copy_of(job, d, r, last).start()

    def receive(job, r, last=False):
        for d in range(4):
            arrival_of(job, d, r, last).wait_recv()

    def pass_on(job, r, last=False):
        for d in range(4):
            arrival_of(job, d, r, False).wait_recv()
            copy_of(job, d, r + 1, last).start()

    def sent(job):
        def one(r, carry):
            for d in range(4):
                copy_of(job, d, r, False).wait_send()
            return carry
        lax.fori_loop(1, ROUNDS, one, 0)
        for d in range(4):
            copy_of(job, d, ROUNDS, True).wait_send()

    for i in range(3):
        loads[i].wait()
    send(WA, 1)
    for i in range(3, 5):
        loads[i].wait()
    send(WG, 1)
    loads[5].wait()

    def norm_rows(i, carry):
        at = pl.ds(pl.multiple_of(i * 64, 64), 64)
        t = tok[at].astype(F32)
        scale = lax.rsqrt(jnp.mean(t * t, axis=-1, keepdims=True) + EPS)
        normed[at] = (t * scale * ngain_ref[...].astype(F32)).astype(BF16)
        return carry

    lax.fori_loop(0, rows // 64, norm_rows, 0)
    for i in range(6, 8):
        loads[i].wait()

    def weights_round(r, carry):
        pass_on(WA, r)
        pass_on(WG, r)
        return carry

    lax.fori_loop(1, ROUNDS - 1, weights_round, 0)
    pass_on(WA, ROUNDS - 1, True)
    pass_on(WG, ROUNDS - 1, True)
    send(WO, 1)
    receive(WA, ROUNDS, True)

    half = rows // 2
    for c in range(2):
        part = dot(normed[pl.ds(c * half, half)], wa[:, pl.ds(0, 256)])
        keys_t = jnp.transpose(part[:, :128]).astype(BF16)
        kv[me * 2 + c, pl.ds(0, 128)] = keys_t[:, :128]
        kv[me * 2 + c, pl.ds(128, 128)] = keys_t[:, 128:]
        kv[me * 2 + c, pl.ds(256, 256)] = part[:, 128:].astype(BF16)
    send(KV, 1)
    for c in range(2):
        at = pl.ds(c * half, half)
        q[at] = dot(normed[at], wa[:, pl.ds(256, 512)]).astype(BF16)

    receive(WG, ROUNDS, True)

    def gate_rows(i, carry):
        at = pl.ds(pl.multiple_of(i * 256, 256), 256)
        value = dot(normed[at], wg[:, pl.ds(0, 512)])
        gate = dot(normed[at], wg[:, pl.ds(512, 512)])
        gated = (value * jax.nn.sigmoid(gate)).astype(BF16).astype(F32)
        for k in range(4):
            gpad[k, pl.ds(pl.multiple_of(32 + i * 256, 32), 256)] = gated[:, k * 128 : k * 128 + 128]
        return carry

    lax.fori_loop(0, rows // 256, gate_rows, 0)
    for k in range(4):
        rim_out[0, k] = gpad[k, pl.ds(rows, 32)].astype(BF16)
    rim = pltpu.make_async_remote_copy(
        src_ref=rim_out.at[0], dst_ref=rim_out.at[1], send_sem=side_send.at[0], recv_sem=side_recv.at[0],
        device_id={"sp": after}, device_id_type=MESH,
    )
    rim.start()

    c_exp = QK ** (-0.5) * math.log2(math.e)

    def keys_of(piece, m):
        k = kv[piece, pl.ds(0, 256)]
        wide = jnp.concatenate([k[:128], k[128:]], axis=1)
        zero = jnp.zeros((QK, 256), BF16)
        return jnp.concatenate([wide[:QK], zero] if m == 0 else [zero, wide[QK:]], axis=0)

    tile = 256

    def attend(piece, diag, first):
        values = kv[piece, pl.ds(256, 256)]
        keys = [keys_of(piece, m) for m in range(2)]

        def one_head(h, carry):
            columns = pl.ds(pl.multiple_of(h * 128, 128), 128)
            for start in range(0, rows, tile):
                if diag is not None and start + tile <= diag:
                    continue
                at = pl.ds(start, tile)
                queries = q[at, columns]
                for m in range(2):
                    w = jnp.exp2(dot(queries, keys[m]) * c_exp)
                    if diag is not None and start < diag + 255:
                        key_pos = diag + lax.broadcasted_iota(jnp.int32, (tile, 256), 1)
                        row_pos = start + lax.broadcasted_iota(jnp.int32, (tile, 256), 0)
                        w = jnp.where(key_pos <= row_pos, w, 0.0)
                    s = w[:, :128] + w[:, 128:]
                    o = dot(w.astype(BF16), values)
                    if first:
                        lsum[h * 2 + m, at] = s
                        acc[h * 2 + m, at] = o
                    else:
                        lsum[h * 2 + m, at] += s
                        acc[h * 2 + m, at] += o
            return carry

        lax.fori_loop(0, 4, one_head, 0)

    def attend_round(r):
        for d in range(4):
            cycle, way = d // 2, d % 2
            sign = 1 if way == 0 else -1
            source = member_at(cycle, places[cycle] - sign * r)

            @pl.when(source < me)
            def _():
                attend(source * 2 + cycle, None, False)

    attend(me * 2, 0, True)
    attend(me * 2 + 1, 256, False)
    pass_on(KV, 1)
    pass_on(WO, 1)

    rim.wait_recv()
    inside = jnp.where(me > 0, 1.0, 0.0)
    for k in range(4):
        gpad[k, pl.ds(0, 32)] = rim_out[1, k].astype(F32) * inside

    def conv_rows_of(i, carry):
        base = pl.multiple_of(i * 64, 64)
        total = jnp.zeros((64, 128), F32)
        for k in range(4):
            out = jnp.zeros((64, 128), F32)
            window = gpad[k, pl.ds(base, 96)]
            for j in range(31):
                out = out + taps_ref[pl.ds(j, 1), pl.ds(k * 128, 128)] * window[j + 2 : j + 66]
            out = out.astype(BF16).astype(F32)
            conv[pl.ds(base, 64), pl.ds(k * 128, 128)] = out
            total = total + out * out
        squares[pl.ds(base, 64)] = total
        return carry

    lax.fori_loop(0, rows // 64, conv_rows_of, 0)
    sq = pltpu.make_async_remote_copy(
        src_ref=squares, dst_ref=sq_in, send_sem=side_send.at[1], recv_sem=side_recv.at[1],
        device_id={"tp": 1 - core}, device_id_type=MESH,
    )
    sq.start()

    def kv_round(r, carry):
        attend_round(r)
        pass_on(KV, r + 1)
        pass_on(WO, r + 1)
        return carry

    lax.fori_loop(1, ROUNDS - 2, kv_round, 0)
    attend_round(ROUNDS - 2)
    pass_on(KV, ROUNDS - 1, True)
    pass_on(WO, ROUNDS - 1, True)
    attend_round(ROUNDS - 1)

    sq.wait_recv()

    def act_rows(i, carry):
        at = pl.ds(pl.multiple_of(i * 64, 64), 64)
        total = jnp.sum(squares[at] + sq_in[at], axis=-1, keepdims=True)
        gain = cgain_ref[:, pl.ds(pl.multiple_of(core * 512, 512), 512)].astype(F32)
        x = conv[at] * lax.rsqrt(total / CONV + EPS) * gain
        both[at, pl.ds(512, 512)] = (x * jax.nn.sigmoid(x)).astype(BF16)
        return carry

    lax.fori_loop(0, rows // 64, act_rows, 0)

    receive(KV, ROUNDS, True)
    for c in range(2):
        source = member_at(c, places[c] + ROUNDS)

        @pl.when(source < me)
        def _():
            attend(source * 2 + c, None, False)

    def finish_rows(i, carry):
        at = pl.ds(pl.multiple_of(i * 64, 64), 64)
        for h in range(4):
            t0 = jnp.sum(lsum[2 * h, at], axis=-1, keepdims=True)
            t1 = jnp.sum(lsum[2 * h + 1, at], axis=-1, keepdims=True)
            diff = acc[2 * h, at] / t0 - lam_ref[h] * acc[2 * h + 1, at] / t1
            out = diff * lax.rsqrt(jnp.mean(diff * diff, axis=-1, keepdims=True) + EPS) * hgain_ref[...].astype(F32)
            both[at, pl.ds(h * 128, 128)] = out.astype(BF16)
            logt_ref[at, pl.ds(2 * h, 1)] = jnp.log(t0)
            logt_ref[at, pl.ds(2 * h + 1, 1)] = jnp.log(t1)
        return carry

    lax.fori_loop(0, rows // 64, finish_rows, 0)
    receive(WO, ROUNDS, True)

    def out_copy(n):
        return pltpu.make_async_remote_copy(
            src_ref=outbox.at[n], dst_ref=inbox.at[n], send_sem=out_send.at[n], recv_sem=out_recv.at[n],
            device_id={"tp": 1 - core}, device_id_type=MESH,
        )

    theirs = pl.ds(pl.multiple_of((1 - core) * 256, 256), 256)
    ours = pl.ds(pl.multiple_of(core * 256, 256), 256)

    def out_columns(n):
        return jnp.concatenate([wo[2 * n], wo[2 * n + 1]], axis=1)

    def their_part(n, carry):
        outbox[n] = dot(both[theirs], out_columns(n)).astype(BF16)
        out_copy(n).start()
        return carry

    lax.fori_loop(0, 8, their_part, 0)

    def our_part(n, carry):
        part = dot(both[ours], out_columns(n))
        out_copy(n).wait_recv()
        mixed_ref[:, pl.ds(pl.multiple_of(n * 256, 256), 256)] = (part + inbox[n].astype(F32)).astype(BF16)
        return carry

    lax.fori_loop(0, 8, our_part, 0)

    for job in range(4):
        sent(job)
    rim.wait_send()
    sq.wait_send()

    def out_sent(n, carry):
        out_copy(n).wait_send()
        return carry

    lax.fori_loop(0, 8, out_sent, 0)


def body(
    tokens, norm_gain, w_query, w_key, w_value, w_glu_value, w_glu_gate, conv_taps, convolution_norm_gain, head_gain, lam, w_out,
):
    rows = tokens.shape[0]
    d = tokens.shape[1]
    vmem = pl.BlockSpec(memory_space=pltpu.VMEM)
    smem = pl.BlockSpec(memory_space=pltpu.SMEM)
    dma = pltpu.SemaphoreType.DMA
    return pl.pallas_call(
        kernel,
        out_shape=(jax.ShapeDtypeStruct((rows // 2, d), BF16), jax.ShapeDtypeStruct((rows, 8), F32)),
        in_specs=[ANY, vmem, ANY, ANY, ANY, ANY, ANY, vmem, vmem, vmem, smem, ANY],
        out_specs=(vmem, vmem),
        scratch_shapes=[
            pltpu.VMEM((rows, d), BF16),
            pltpu.VMEM((rows, d), BF16),
            pltpu.VMEM((d, 768), BF16),
            pltpu.VMEM((d, 1024), BF16),
            pltpu.VMEM((RING, 1024, 128), BF16),
            pltpu.VMEM((2 * RING, 512, 128), BF16),
            pltpu.VMEM((rows, 512), BF16),
            pltpu.VMEM((8, rows, 128), F32),
            pltpu.VMEM((8, rows, 128), F32),
            pltpu.VMEM((4, rows + 32, 128), F32),
            pltpu.VMEM((rows, 512), F32),
            pltpu.VMEM((rows, 128), F32),
            pltpu.VMEM((rows, 1024), BF16),
            pltpu.VMEM((8, 256, 256), BF16),
            pltpu.VMEM((8, 256, 256), BF16),
            pltpu.VMEM((2, 4, 32, 128), BF16),
            pltpu.VMEM((rows, 128), F32),
            dma((8,)),
            dma((4, 4, ROUNDS)),
            dma((4, 4, ROUNDS)),
            dma((2,)),
            dma((2,)),
            dma((8,)),
            dma((8,)),
        ],
        compiler_params=pltpu.CompilerParams(
            collective_id=0, has_side_effects=True, vmem_limit_bytes=60 * 1024 * 1024
        ),
    )(
        tokens, norm_gain.reshape(1, -1), w_query, w_key, w_value, w_glu_value, w_glu_gate,
        conv_taps.astype(F32), convolution_norm_gain.reshape(1, -1), head_gain.reshape(1, -1), lam, w_out,
    )


def solution(mesh):
    return jax.shard_map(
        body,
        mesh=mesh,
        in_specs=(
            P(("fs", "sp"), None),
            P(),
            P("sp", "tp"),
            P("sp", "tp"),
            P("sp", "tp"),
            P("sp", "tp"),
            P("sp", "tp"),
            P(None, "tp"),
            P(),
            P(),
            P("tp"),
            P(None, "sp"),
        ),
        out_specs=(P(("fs", "sp", "tp"), None), P(("fs", "sp"), "tp")),
        check_vma=False,
    )
```

```python
import functools
import math

import jax
import jax.numpy as jnp
from jax import lax
from jax.experimental import pallas as pl
from jax.experimental.pallas import tpu as pltpu
from jax.sharding import PartitionSpec as P

HEADS = 8
QK = 64
VDIM = 128
CONV = 1024
EPS = 1e-06
RING = 16
MESH = pl.DeviceIdType.MESH
ANY = pl.BlockSpec(memory_space=pl.ANY)
F32 = jnp.float32
BF16 = jnp.bfloat16


def dot(a, b):
    return jnp.dot(a, b, preferred_element_type=F32)


KINDS = ("u1", "u2", "v0", "vm", "vp", "q0", "q1", "f0", "fm", "fp", "f2")
WAYS = ((0, 1), (1, -1))


def kernel(
    tok_hbm, ngain_ref, wq_hbm, wk_hbm, wv_hbm, wgv_hbm, wgg_hbm, taps_ref, cgain_ref, hgain_ref, lam_ref, wout_hbm,
    mixed_ref, logt_ref,
    tok, normed, wa, wg, wo, kv, q, acc, lsum, gpad, conv, squares, both, outbox, inbox, rim_box, sq_in, taps,
    load_sem, send_sem, recv_sem, plane_send, plane_recv, side_send, side_recv, out_send, out_recv,
):
    rows = tok.shape[0]
    me = lax.axis_index("sp")
    core = lax.axis_index("tp")
    plane = lax.axis_index("fs")
    mine_z, mine_x = lax.div(me, 4), lax.rem(me, 4)
    after, before = lax.rem(me + 1, RING), lax.rem(me + RING - 1, RING)
    planes = [lax.rem(plane + 1, 4), lax.rem(plane + 3, 4)]

    def at_offset(dx, dz):
        return lax.rem(mine_z + dz + 8, 4) * 4 + lax.rem(mine_x + dx + 8, 4)

    def offset(c, du, dv):
        return at_offset(du, dv) if c == 0 else at_offset(dv, du)

    mine = pl.ds(pl.multiple_of(me * 128, 128), 128)
    quarter = pl.ds(pl.multiple_of(plane * 256, 256), 256)
    out_from = lax.div(plane, 2) * 1024 + core * 512 + lax.rem(plane, 2) * 256
    loads = [
        (wk_hbm, wa.at[mine, pl.ds(0, 128)]),
        (wv_hbm, wa.at[mine, pl.ds(128, 128)]),
        (wq_hbm, wa.at[mine, pl.ds(256, 512)]),
        (wout_hbm.at[pl.ds(pl.multiple_of(out_from, 256), 256)], wo.at[me, quarter]),
        (tok_hbm, tok),
        (wgv_hbm, wg.at[mine, pl.ds(0, 512)]),
        (wgg_hbm, wg.at[mine, pl.ds(512, 512)]),
    ]
    loads = [pltpu.make_async_copy(s, d, load_sem.at[i]) for i, (s, d) in enumerate(loads)]
    for load in loads:
        load.start()

    barrier = pltpu.get_barrier_semaphore()
    for peer in [offset(c, s, 0) for c in range(2) for _, s in WAYS] + [after, before]:
        pl.semaphore_signal(barrier, inc=1, device_id={"sp": peer}, device_id_type=MESH)
    for peer in planes:
        pl.semaphore_signal(barrier, inc=1, device_id={"fs": peer}, device_id_type=MESH)
    pl.semaphore_signal(barrier, inc=1, device_id={"tp": 1 - core}, device_id_type=MESH)
    pl.semaphore_wait(barrier, 9)

    def weight_rows(ref):
        def part(source, c, at, size):
            start = source * 128 + c * 64 + at * 32
            return ref.at[pl.ds(pl.multiple_of(start, 32), size * 32)]
        return part

    def out_rows(source, c, at, size):
        start = plane * 256 + c * 128 + at * 64
        return wo.at[source, pl.ds(pl.multiple_of(start, 64), size * 64)]

    def kv_rows(source, c, at, size):
        return kv.at[source * 2 + c, pl.ds(at * 256, size * 256)]

    jobs = [weight_rows(wa), weight_rows(wg), kv_rows, out_rows]
    WA, WG, KV, WO = range(4)

    def message(job, c, w, kind, arriving=False):
        sign = WAYS[w][1]
        along = kind[0] == "u"
        du = {"u1": 0, "u2": -sign, "v0": 0, "f0": 0, "vm": -1, "fm": -1, "vp": 1, "fp": 1, "q0": 2, "q1": 2, "f2": 2}[kind]
        dv = -sign if kind[0] == "f" else 0
        at, size = {"u1": (0, 2), "v0": (0, 2), "vm": (0, 2), "vp": (0, 2), "q0": (0, 1), "q1": (1, 1)}.get(kind, (w, 1))
        peer = offset(c, sign, 0) if along else offset(c, 0, sign)
        if arriving:
            du, dv = (du - sign, dv) if along else (du, dv - sign)
        ref = jobs[job](offset(c, du, dv), c, at, size)
        k = KINDS.index(kind)
        return pltpu.make_async_remote_copy(
            src_ref=ref, dst_ref=ref, send_sem=send_sem.at[job, c, w, k], recv_sem=recv_sem.at[job, c, w, k],
            device_id={"sp": peer}, device_id_type=MESH,
        )

    def go(job, c, w, kind):
        message(job, c, w, kind).start()

    def come(job, c, w, kind):
        message(job, c, w, kind, True).wait_recv()

    BOTH = ((0, 0), (0, 1), (1, 0), (1, 1))

    def step0(job):
        for c, w in BOTH:
            go(job, c, w, "u1")
        for c, w in BOTH:
            go(job, c, w, "v0")

    def step1(job):
        for c, w in BOTH:
            come(job, c, w, "u1")
            go(job, c, w, "u2")
            for w2 in range(2):
                go(job, c, w2, "vm" if w == 0 else "vp")
        for c, w in BOTH:
            come(job, c, w, "v0")
            go(job, c, w, "f0")

    def step2(job):
        for c, w in BOTH:
            come(job, c, w, "u2")
            for w2 in range(2):
                go(job, c, w2, "q0" if w == 0 else "q1")
        for c, w in BOTH:
            for side in "mp":
                come(job, c, w, "v" + side)
                go(job, c, w, "f" + side)
        for c, w in BOTH:
            come(job, c, w, "f0")

    def step3(job):
        for c, w in BOTH:
            come(job, c, w, "q0")
            come(job, c, w, "q1")
            go(job, c, w, "f2")
        for c, w in BOTH:
            come(job, c, w, "fm")
            come(job, c, w, "fp")

    def step4(job):
        for c, w in BOTH:
            come(job, c, w, "f2")

    def plane_message(b, w, forward, arriving=False):
        sign = WAYS[w][1]
        back = (1 if forward else 0) + (1 if arriving else 0)
        quarter = lax.rem(plane - sign * back + 8, 4)
        start = quarter * 256 + (w * 128 if forward else 0)
        ref = wo.at[pl.ds(4 * b, 4), pl.ds(pl.multiple_of(start, 128), 128 if forward else 256)]
        k = 4 * b + 2 * w + (1 if forward else 0)
        return pltpu.make_async_remote_copy(
            src_ref=ref, dst_ref=ref, send_sem=plane_send.at[k], recv_sem=plane_recv.at[k],
            device_id={"fs": planes[w]}, device_id_type=MESH,
        )

    def planes_start():
        for b in range(4):
            for w in range(2):
                plane_message(b, w, False).start()

    def planes_forward(b):
        for w in range(2):
            plane_message(b, w, False, True).wait_recv()
            plane_message(b, w, True).start()

    for i in range(3):
        loads[i].wait()
    step0(WA)
    loads[3].wait()
    step0(WO)
    loads[4].wait()

    def norm_rows(i, carry):
        at = pl.ds(pl.multiple_of(i * 64, 64), 64)
        t = tok[at].astype(F32)
        scale = lax.rsqrt(jnp.mean(t * t, axis=-1, keepdims=True) + EPS)
        normed[at] = (t * scale * ngain_ref[...].astype(F32).reshape(1, -1)).astype(BF16)
        return carry

    step1(WA)
    step1(WO)
    lax.fori_loop(0, rows // 64, norm_rows, 0)
    step2(WA)
    step2(WO)
    step3(WA)
    for i in range(5, 7):
        loads[i].wait()
    step0(WG)
    taps[...] = taps_ref[...].astype(F32)
    step3(WO)
    step4(WA)

    half = rows // 2
    for c in range(2):
        part = dot(normed[pl.ds(c * half, half)], wa[:, pl.ds(0, 256)])
        keys_t = jnp.transpose(part[:, :128]).astype(BF16)
        kv[me * 2 + c, pl.ds(0, 128)] = keys_t[:, :128]
        kv[me * 2 + c, pl.ds(128, 128)] = keys_t[:, 128:]
        kv[me * 2 + c, pl.ds(256, 256)] = part[:, 128:].astype(BF16)
    step0(KV)
    step4(WO)
    planes_start()
    for c in range(2):
        at = pl.ds(c * half, half)
        q[at] = dot(normed[at], wa[:, pl.ds(256, 512)]).astype(BF16)

    c_exp = QK ** (-0.5) * math.log2(math.e)

    def keys_of(pieces, m):
        parts = []
        for piece in pieces:
            k = kv[piece, pl.ds(0, 256)]
            parts += [k[:128], k[128:]]
        wide = jnp.concatenate(parts, axis=1)
        zero = jnp.zeros((QK, wide.shape[1]), BF16)
        return jnp.concatenate([wide[:QK], zero] if m == 0 else [zero, wide[QK:]], axis=0)

    def lane_sum(w):
        s = w[:, :128]
        for k in range(1, w.shape[1] // 128):
            s = s + w[:, k * 128 : k * 128 + 128]
        return s

    def attend_source(source):
        pieces = [source * 2, source * 2 + 1]
        values = jnp.concatenate([kv[p, pl.ds(256, 256)] for p in pieces], axis=0)
        keys = [keys_of(pieces, m) for m in range(2)]
        for h in range(4):
            queries = q[:, pl.ds(h * 128, 128)]
            for m in range(2):
                w = jnp.exp2(dot(queries, keys[m]) * c_exp)
                s = lane_sum(w)
                o = dot(w.astype(BF16), values)
                lsum[h * 2 + m] += s
                acc[h * 2 + m] += o

    def attend_own(c):
        start = c * half
        pieces = [me * 2, me * 2 + 1][: c + 1]
        values = jnp.concatenate([kv[p, pl.ds(256, 256)] for p in pieces], axis=0)
        keys = [keys_of(pieces, m) for m in range(2)]
        at = pl.ds(start, half)
        width = 256 * len(pieces)
        key_pos = lax.broadcasted_iota(jnp.int32, (half, width), 1)
        row_pos = start + lax.broadcasted_iota(jnp.int32, (half, width), 0)
        for h in range(4):
            queries = q[at, pl.ds(h * 128, 128)]
            for m in range(2):
                w = jnp.exp2(dot(queries, keys[m]) * c_exp)
                w = jnp.where(key_pos <= row_pos, w, 0.0)
                lsum[h * 2 + m, at] = lane_sum(w)
                acc[h * 2 + m, at] = dot(w.astype(BF16), values)

    def attend_group(count, where):
        def one(i, carry):
            dx, dz = where(i)
            source = at_offset(dx, dz)

            @pl.when(source < me)
            def _():
                attend_source(source)
            return carry

        lax.fori_loop(0, count, one, 0)

    def odd(i):
        return 1 + 2 * lax.rem(i, 2)

    for c in range(2):
        attend_own(c)
    step1(KV)
    step1(WG)
    attend_group(4, lambda i: ((1 - lax.div(i, 2)) * odd(i), lax.div(i, 2) * odd(i)))
    step2(KV)
    step2(WG)
    planes_forward(0)
    attend_group(4, lambda i: (1 + 2 * lax.div(i, 2), odd(i)))
    step3(KV)
    planes_forward(1)
    attend_group(2, lambda i: (2 * (1 - i), 2 * i))
    step3(WG)
    planes_forward(2)
    attend_group(
        4,
        lambda i: (
            2 * (1 - lax.div(i, 2)) + lax.div(i, 2) * odd(i),
            2 * lax.div(i, 2) + (1 - lax.div(i, 2)) * odd(i),
        ),
    )
    planes_forward(3)

    step4(WG)

    def gate_rows(i, carry):
        at = pl.ds(pl.multiple_of(i * 256, 256), 256)
        value = dot(normed[at], wg[:, pl.ds(0, 512)])
        gate = dot(normed[at], wg[:, pl.ds(512, 512)])
        gated = (value * jax.nn.sigmoid(gate)).astype(BF16).astype(F32)
        for k in range(4):
            gpad[k, pl.ds(pl.multiple_of(32 + i * 256, 32), 256)] = gated[:, k * 128 : k * 128 + 128]
        return carry

    lax.fori_loop(0, rows // 256, gate_rows, 0)
    for k in range(4):
        rim_box[0, k] = gpad[k, pl.ds(rows, 32)].astype(BF16)
    rim = pltpu.make_async_remote_copy(
        src_ref=rim_box.at[0], dst_ref=rim_box.at[1], send_sem=side_send.at[0], recv_sem=side_recv.at[0],
        device_id={"sp": after}, device_id_type=MESH,
    )
    rim.start()

    step4(KV)
    attend_group(1, lambda i: (2, 2))

    def finish_rows(i, carry):
        at = pl.ds(pl.multiple_of(i * 128, 128), 128)
        lane = lax.broadcasted_iota(jnp.int32, (128, 128), 1)
        logs = jnp.zeros((128, 128), F32)
        for h in range(4):
            t0 = jnp.sum(lsum[2 * h, at], axis=-1, keepdims=True)
            t1 = jnp.sum(lsum[2 * h + 1, at], axis=-1, keepdims=True)
            diff = acc[2 * h, at] / t0 - lam_ref[h] * acc[2 * h + 1, at] / t1
            out = diff * lax.rsqrt(jnp.mean(diff * diff, axis=-1, keepdims=True) + EPS) * hgain_ref[...].astype(F32)
            both[at, pl.ds(h * 128, 128)] = out.astype(BF16)
            logs = jnp.where(lane == 2 * h, t0, logs)
            logs = jnp.where(lane == 2 * h + 1, t1, logs)
        logt_ref[:, at] = jnp.log(jnp.transpose(logs)[:8])
        return carry

    lax.fori_loop(0, rows // 128, finish_rows, 0)

    rim.wait_recv()
    inside = jnp.where(me > 0, 1.0, 0.0)
    for k in range(4):
        gpad[k, pl.ds(0, 32)] = rim_box[1, k].astype(F32) * inside

    def conv_rows_of(i, carry):
        base = pl.multiple_of(i * 64, 64)
        total = jnp.zeros((64, 128), F32)
        for k in range(4):
            out = jnp.zeros((64, 128), F32)
            window = gpad[k, pl.ds(base, 96)]
            for j in range(31):
                out = out + taps[pl.ds(j, 1), pl.ds(k * 128, 128)] * window[j + 2 : j + 66]
            out = out.astype(BF16).astype(F32)
            conv[pl.ds(base, 64), pl.ds(k * 128, 128)] = out
            total = total + out * out
        squares[pl.ds(base, 64)] = total
        return carry

    lax.fori_loop(0, rows // 64, conv_rows_of, 0)
    sq = pltpu.make_async_remote_copy(
        src_ref=squares, dst_ref=sq_in, send_sem=side_send.at[1], recv_sem=side_recv.at[1],
        device_id={"tp": 1 - core}, device_id_type=MESH,
    )
    sq.start()
    for b in range(4):
        for w in range(2):
            plane_message(b, w, True, True).wait_recv()
    sq.wait_recv()

    def act_rows(i, carry):
        at = pl.ds(pl.multiple_of(i * 64, 64), 64)
        total = jnp.sum(squares[at] + sq_in[at], axis=-1, keepdims=True)
        gain = cgain_ref[pl.ds(pl.multiple_of(core * 512, 512), 512)].astype(F32).reshape(1, 512)
        x = conv[at] * lax.rsqrt(total / CONV + EPS) * gain
        both[at, pl.ds(512, 512)] = (x * jax.nn.sigmoid(x)).astype(BF16)
        return carry

    lax.fori_loop(0, rows // 64, act_rows, 0)

    def out_copy(n):
        return pltpu.make_async_remote_copy(
            src_ref=outbox.at[n], dst_ref=inbox.at[n], send_sem=out_send.at[n], recv_sem=out_recv.at[n],
            device_id={"tp": 1 - core}, device_id_type=MESH,
        )

    theirs = pl.ds(pl.multiple_of((1 - core) * 256, 256), 256)
    ours = pl.ds(pl.multiple_of(core * 256, 256), 256)

    def out_columns(n):
        return jnp.concatenate([wo[2 * n], wo[2 * n + 1]], axis=1)

    def their_part(n, carry):
        outbox[n] = dot(both[theirs], out_columns(n)).astype(BF16)
        out_copy(n).start()
        return carry

    lax.fori_loop(0, 8, their_part, 0)

    def our_part(n, carry):
        part = dot(both[ours], out_columns(n))
        out_copy(n).wait_recv()
        mixed_ref[:, pl.ds(pl.multiple_of(n * 256, 256), 256)] = (part + inbox[n].astype(F32)).astype(BF16)
        return carry

    lax.fori_loop(0, 8, our_part, 0)

    for job in range(4):
        for c, w in BOTH:
            for kind in KINDS:
                message(job, c, w, kind).wait_send()
    for b in range(4):
        for w in range(2):
            plane_message(b, w, False).wait_send()
            plane_message(b, w, True).wait_send()
    rim.wait_send()
    sq.wait_send()

    def out_sent(n, carry):
        out_copy(n).wait_send()
        return carry

    lax.fori_loop(0, 8, out_sent, 0)


def body(
    tokens, norm_gain, w_query, w_key, w_value, w_glu_value, w_glu_gate, conv_taps, convolution_norm_gain, head_gain, lam, w_out,
):
    rows = tokens.shape[0]
    d = tokens.shape[1]
    vmem = pl.BlockSpec(memory_space=pltpu.VMEM)
    smem = pl.BlockSpec(memory_space=pltpu.SMEM)
    dma = pltpu.SemaphoreType.DMA
    mixed, logs = pl.pallas_call(
        kernel,
        out_shape=(jax.ShapeDtypeStruct((rows // 2, d), BF16), jax.ShapeDtypeStruct((8, rows), F32)),
        in_specs=[ANY, vmem, ANY, ANY, ANY, ANY, ANY, vmem, vmem, vmem, smem, ANY],
        out_specs=(vmem, vmem),
        scratch_shapes=[
            pltpu.VMEM((rows, d), BF16),
            pltpu.VMEM((rows, d), BF16),
            pltpu.VMEM((d, 768), BF16),
            pltpu.VMEM((d, 1024), BF16),
            pltpu.VMEM((RING, 1024, 128), BF16),
            pltpu.VMEM((2 * RING, 512, 128), BF16),
            pltpu.VMEM((rows, 512), BF16),
            pltpu.VMEM((8, rows, 128), F32),
            pltpu.VMEM((8, rows, 128), F32),
            pltpu.VMEM((4, rows + 32, 128), F32),
            pltpu.VMEM((rows, 512), F32),
            pltpu.VMEM((rows, 128), F32),
            pltpu.VMEM((rows, 1024), BF16),
            pltpu.VMEM((8, 256, 256), BF16),
            pltpu.VMEM((8, 256, 256), BF16),
            pltpu.VMEM((2, 4, 32, 128), BF16),
            pltpu.VMEM((rows, 128), F32),
            pltpu.VMEM((31, 512), F32),
            dma((7,)),
            dma((4, 2, 2, len(KINDS))),
            dma((4, 2, 2, len(KINDS))),
            dma((16,)),
            dma((16,)),
            dma((2,)),
            dma((2,)),
            dma((8,)),
            dma((8,)),
        ],
        compiler_params=pltpu.CompilerParams(
            collective_id=0, has_side_effects=True, vmem_limit_bytes=60 * 1024 * 1024
        ),
    )(
        tokens, norm_gain, w_query, w_key, w_value, w_glu_value, w_glu_gate,
        conv_taps, convolution_norm_gain, head_gain.reshape(1, -1), lam, w_out,
    )
    return mixed, logs.T


def solution(mesh):
    return jax.shard_map(
        body,
        mesh=mesh,
        in_specs=(
            P(("fs", "sp"), None),
            P(),
            P("sp", "tp"),
            P("sp", "tp"),
            P("sp", "tp"),
            P("sp", "tp"),
            P("sp", "tp"),
            P(None, "tp"),
            P(),
            P(),
            P("tp"),
            P(None, "sp"),
        ),
        out_specs=(P(("fs", "sp", "tp"), None), P(("fs", "sp"), "tp")),
        check_vma=False,
    )
```

```python
import functools
import math

import jax
import jax.numpy as jnp
from jax import lax
from jax.experimental import pallas as pl
from jax.experimental.pallas import tpu as pltpu
from jax.sharding import PartitionSpec as P

HEADS = 8
QK = 64
VDIM = 128
CONV = 1024
EPS = 1e-06
RING = 16
MESH = pl.DeviceIdType.MESH
ANY = pl.BlockSpec(memory_space=pl.ANY)
F32 = jnp.float32
BF16 = jnp.bfloat16


def dot(a, b):
    return jnp.dot(a, b, preferred_element_type=F32)


KINDS = ("u1", "u2", "v0", "vm", "vp", "q0", "q1", "f0", "fm", "fp", "f2")
WAYS = ((0, 1), (1, -1))


def kernel(
    tok_hbm, ngain_ref, wq_hbm, wk_hbm, wv_hbm, wgv_hbm, wgg_hbm, taps_ref, cgain_ref, hgain_ref, lam_ref, wout_hbm,
    mixed_ref, logt_ref,
    tok, normed, wkv, wq, wg, wo, kv, q, acc, lsum, gpad, conv, squares, both, outbox, inbox, rim_box, sq_in, taps,
    load_sem, send_sem, recv_sem, plane_send, plane_recv, side_send, side_recv, out_send, out_recv,
):
    rows = tok.shape[0]
    me = lax.axis_index("sp")
    core = lax.axis_index("tp")
    plane = lax.axis_index("fs")
    mine_z, mine_x = lax.div(me, 4), lax.rem(me, 4)
    after, before = lax.rem(me + 1, RING), lax.rem(me + RING - 1, RING)
    planes = [lax.rem(plane + 1, 4), lax.rem(plane + 3, 4)]

    def at_offset(dx, dz):
        return lax.rem(mine_z + dz + 8, 4) * 4 + lax.rem(mine_x + dx + 8, 4)

    def offset(c, du, dv):
        return at_offset(du, dv) if c == 0 else at_offset(dv, du)

    mine = pl.ds(pl.multiple_of(me * 128, 128), 128)
    quarter = pl.ds(pl.multiple_of(plane * 128, 128), 128)
    att_rows = pl.ds(pl.multiple_of(core * 512, 512), 512)
    conv_rows = pl.ds(pl.multiple_of(1024 + core * 512, 512), 512)
    loads = [
        (wk_hbm, wkv.at[mine, pl.ds(0, 128)]),
        (wv_hbm, wkv.at[mine, pl.ds(128, 128)]),
        (wq_hbm, wq.at[mine]),
        (wgv_hbm.at[:, quarter], wg.at[plane, 0, mine]),
        (wgg_hbm.at[:, quarter], wg.at[plane, 1, mine]),
        (tok_hbm, tok),
        (wout_hbm.at[att_rows], wo.at[me, pl.ds(0, 512)]),
        (wout_hbm.at[conv_rows], wo.at[me, pl.ds(512, 512)]),
    ]
    loads = [pltpu.make_async_copy(s, d, load_sem.at[i]) for i, (s, d) in enumerate(loads)]
    for load in loads:
        load.start()

    barrier = pltpu.get_barrier_semaphore()
    for peer in [offset(c, s, 0) for c in range(2) for _, s in WAYS] + [after, before]:
        pl.semaphore_signal(barrier, inc=1, device_id={"sp": peer}, device_id_type=MESH)
    for peer in planes:
        pl.semaphore_signal(barrier, inc=1, device_id={"fs": peer}, device_id_type=MESH)
    pl.semaphore_signal(barrier, inc=1, device_id={"tp": 1 - core}, device_id_type=MESH)
    pl.semaphore_wait(barrier, 9)

    def weight_rows(ref):
        def part(source, c, at, size):
            start = source * 128 + c * 64 + at * 32
            return ref.at[pl.ds(pl.multiple_of(start, 32), size * 32)]
        return part

    def glu_rows(source, c, at, size):
        start = source * 128 + c * 64 + at * 32
        return wg.at[plane, :, pl.ds(pl.multiple_of(start, 32), size * 32)]

    def out_rows(first):
        def part(source, c, at, size):
            return wo.at[source, pl.ds(first + c * 256 + at * 128, size * 128)]
        return part

    def kv_rows(source, c, at, size):
        return kv.at[source * 2 + c, pl.ds(at * 256, size * 256)]

    jobs = [weight_rows(wkv), weight_rows(wq), glu_rows, kv_rows, out_rows(0), out_rows(512)]
    WKV, WQ, WG, KV, WOA, WOB = range(6)

    def message(job, c, w, kind, arriving=False):
        sign = WAYS[w][1]
        along = kind[0] == "u"
        du = {"u1": 0, "u2": -sign, "v0": 0, "f0": 0, "vm": -1, "fm": -1, "vp": 1, "fp": 1, "q0": 2, "q1": 2, "f2": 2}[kind]
        dv = -sign if kind[0] == "f" else 0
        at, size = {"u1": (0, 2), "v0": (0, 2), "vm": (0, 2), "vp": (0, 2), "q0": (0, 1), "q1": (1, 1)}.get(kind, (w, 1))
        peer = offset(c, sign, 0) if along else offset(c, 0, sign)
        if arriving:
            du, dv = (du - sign, dv) if along else (du, dv - sign)
        ref = jobs[job](offset(c, du, dv), c, at, size)
        k = KINDS.index(kind)
        return pltpu.make_async_remote_copy(
            src_ref=ref, dst_ref=ref, send_sem=send_sem.at[job, c, w, k], recv_sem=recv_sem.at[job, c, w, k],
            device_id={"sp": peer}, device_id_type=MESH,
        )

    def go(job, c, w, kind):
        message(job, c, w, kind).start()

    def come(job, c, w, kind):
        message(job, c, w, kind, True).wait_recv()

    BOTH = ((0, 0), (0, 1), (1, 0), (1, 1))

    def step0(job):
        for c, w in BOTH:
            go(job, c, w, "u1")
        for c, w in BOTH:
            go(job, c, w, "v0")

    def step1(job):
        for c, w in BOTH:
            come(job, c, w, "u1")
            go(job, c, w, "u2")
            for w2 in range(2):
                go(job, c, w2, "vm" if w == 0 else "vp")
        for c, w in BOTH:
            come(job, c, w, "v0")
            go(job, c, w, "f0")

    def step2(job):
        for c, w in BOTH:
            come(job, c, w, "u2")
            for w2 in range(2):
                go(job, c, w2, "q0" if w == 0 else "q1")
        for c, w in BOTH:
            for side in "mp":
                come(job, c, w, "v" + side)
                go(job, c, w, "f" + side)
        for c, w in BOTH:
            come(job, c, w, "f0")

    def step3(job):
        for c, w in BOTH:
            come(job, c, w, "q0")
            come(job, c, w, "q1")
            go(job, c, w, "f2")
        for c, w in BOTH:
            come(job, c, w, "fm")
            come(job, c, w, "fp")

    def step4(job):
        for c, w in BOTH:
            come(job, c, w, "f2")

    def plane_message(b, w, forward, arriving=False):
        sign = WAYS[w][1]
        back = (1 if forward else 0) + (1 if arriving else 0)
        owner = lax.rem(plane - sign * back + 8, 4)
        start = b * 512 + (w * 256 if forward else 0)
        ref = wg.at[owner, :, pl.ds(start, 256 if forward else 512)]
        k = 4 * b + 2 * w + (1 if forward else 0)
        return pltpu.make_async_remote_copy(
            src_ref=ref, dst_ref=ref, send_sem=plane_send.at[k], recv_sem=plane_recv.at[k],
            device_id={"fs": planes[w]}, device_id_type=MESH,
        )

    def planes_start():
        for b in range(4):
            for w in range(2):
                plane_message(b, w, False).start()

    def planes_forward(b):
        for w in range(2):
            plane_message(b, w, False, True).wait_recv()
            plane_message(b, w, True).start()

    half = rows // 2

    def norm_rows(i, carry):
        at = pl.ds(pl.multiple_of(i * 64, 64), 64)
        t = tok[at].astype(F32)
        scale = lax.rsqrt(jnp.mean(t * t, axis=-1, keepdims=True) + EPS)
        normed[at] = (t * scale * ngain_ref[...].astype(F32).reshape(1, -1)).astype(BF16)
        return carry

    c_exp = QK ** (-0.5) * math.log2(math.e)

    def keys_of(pieces, m):
        parts = []
        for piece in pieces:
            k = kv[piece, pl.ds(0, 256)]
            parts += [k[:128], k[128:]]
        wide = jnp.concatenate(parts, axis=1)
        zero = jnp.zeros((QK, wide.shape[1]), BF16)
        return jnp.concatenate([wide[:QK], zero] if m == 0 else [zero, wide[QK:]], axis=0)

    def lane_sum(w):
        s = w[:, :128]
        for k in range(1, w.shape[1] // 128):
            s = s + w[:, k * 128 : k * 128 + 128]
        return s

    def attend_source(source):
        pieces = [source * 2, source * 2 + 1]
        values = jnp.concatenate([kv[p, pl.ds(256, 256)] for p in pieces], axis=0)
        keys = [keys_of(pieces, m) for m in range(2)]
        for h in range(4):
            queries = q[:, pl.ds(h * 128, 128)]
            for m in range(2):
                w = jnp.exp2(dot(queries, keys[m]) * c_exp)
                s = lane_sum(w)
                o = dot(w.astype(BF16), values)
                lsum[h * 2 + m] += s
                acc[h * 2 + m] += o

    def attend_own(c):
        start = c * half
        pieces = [me * 2, me * 2 + 1][: c + 1]
        values = jnp.concatenate([kv[p, pl.ds(256, 256)] for p in pieces], axis=0)
        keys = [keys_of(pieces, m) for m in range(2)]
        at = pl.ds(start, half)
        width = 256 * len(pieces)
        key_pos = lax.broadcasted_iota(jnp.int32, (half, width), 1)
        row_pos = start + lax.broadcasted_iota(jnp.int32, (half, width), 0)
        for h in range(4):
            queries = q[at, pl.ds(h * 128, 128)]
            for m in range(2):
                w = jnp.exp2(dot(queries, keys[m]) * c_exp)
                w = jnp.where(key_pos <= row_pos, w, 0.0)
                lsum[h * 2 + m, at] = lane_sum(w)
                acc[h * 2 + m, at] = dot(w.astype(BF16), values)

    def attend_group(first, count, where):
        def one(i, carry):
            dx, dz = where(i)
            source = at_offset(dx, dz)

            @pl.when(source < me)
            def _():
                attend_source(source)
            return carry

        lax.fori_loop(first, first + count, one, 0)

    def odd(i):
        return 1 + 2 * lax.rem(i, 2)

    def straight(i):
        return (1 - lax.div(i, 2)) * odd(i), lax.div(i, 2) * odd(i)

    def corner(i):
        return 1 + 2 * lax.div(i, 2), odd(i)

    def opposite(i):
        return 2 * (1 - i), 2 * i

    def knight(i):
        side = lax.div(i, 2)
        return 2 * (1 - side) + side * odd(i), 2 * side + (1 - side) * odd(i)

    def gate_rows(i, carry):
        at = pl.ds(pl.multiple_of(i * 256, 256), 256)
        value = dot(normed[at], jnp.concatenate([wg[k, 0] for k in range(4)], axis=1))
        gate = dot(normed[at], jnp.concatenate([wg[k, 1] for k in range(4)], axis=1))
        gated = (value * jax.nn.sigmoid(gate)).astype(BF16).astype(F32)
        for k in range(4):
            gpad[k, pl.ds(pl.multiple_of(32 + i * 256, 32), 256)] = gated[:, k * 128 : k * 128 + 128]
        return carry

    rim = pltpu.make_async_remote_copy(
        src_ref=rim_box.at[0], dst_ref=rim_box.at[1], send_sem=side_send.at[0], recv_sem=side_recv.at[0],
        device_id={"sp": after}, device_id_type=MESH,
    )

    def finish_rows(i, carry):
        at = pl.ds(pl.multiple_of(i * 128, 128), 128)
        lane = lax.broadcasted_iota(jnp.int32, (128, 128), 1)
        logs = jnp.zeros((128, 128), F32)
        for h in range(4):
            t0 = jnp.sum(lsum[2 * h, at], axis=-1, keepdims=True)
            t1 = jnp.sum(lsum[2 * h + 1, at], axis=-1, keepdims=True)
            diff = acc[2 * h, at] / t0 - lam_ref[h] * acc[2 * h + 1, at] / t1
            out = diff * lax.rsqrt(jnp.mean(diff * diff, axis=-1, keepdims=True) + EPS) * hgain_ref[...].astype(F32)
            both[at, pl.ds(h * 128, 128)] = out.astype(BF16)
            logs = jnp.where(lane == 2 * h, t0, logs)
            logs = jnp.where(lane == 2 * h + 1, t1, logs)
        logt_ref[:, at] = jnp.log(jnp.transpose(logs)[:8])
        return carry


    def conv_rows_of(i, carry):
        base = pl.multiple_of(i * 64, 64)
        total = jnp.zeros((64, 128), F32)
        for k in range(4):
            out = jnp.zeros((64, 128), F32)
            window = gpad[k, pl.ds(base, 96)]
            for j in range(31):
                out = out + taps[pl.ds(j, 1), pl.ds(k * 128, 128)] * window[j + 2 : j + 66]
            out = out.astype(BF16).astype(F32)
            conv[pl.ds(base, 64), pl.ds(k * 128, 128)] = out
            total = total + out * out
        squares[pl.ds(base, 64)] = total
        return carry

    sq = pltpu.make_async_remote_copy(
        src_ref=squares, dst_ref=sq_in, send_sem=side_send.at[1], recv_sem=side_recv.at[1],
        device_id={"tp": 1 - core}, device_id_type=MESH,
    )

    def act_rows(i, carry):
        at = pl.ds(pl.multiple_of(i * 64, 64), 64)
        total = jnp.sum(squares[at] + sq_in[at], axis=-1, keepdims=True)
        gain = cgain_ref[pl.ds(pl.multiple_of(core * 512, 512), 512)].astype(F32).reshape(1, 512)
        x = conv[at] * lax.rsqrt(total / CONV + EPS) * gain
        both[at, pl.ds(512, 512)] = (x * jax.nn.sigmoid(x)).astype(BF16)
        return carry

    def out_copy(n):
        return pltpu.make_async_remote_copy(
            src_ref=outbox.at[n], dst_ref=inbox.at[n], send_sem=out_send.at[n], recv_sem=out_recv.at[n],
            device_id={"tp": 1 - core}, device_id_type=MESH,
        )

    theirs = pl.ds(pl.multiple_of((1 - core) * 256, 256), 256)
    ours = pl.ds(pl.multiple_of(core * 256, 256), 256)

    def out_columns(n):
        return jnp.concatenate([wo[8 * n + k] for k in range(8)], axis=1)

    loads[0].wait()
    loads[1].wait()
    step0(WKV)
    loads[3].wait()
    loads[4].wait()
    step0(WG)
    loads[5].wait()
    lax.fori_loop(0, rows // 64, norm_rows, 0)
    taps[...] = taps_ref[...].astype(F32)
    loads[2].wait()
    step0(WQ)
    step1(WKV)
    step1(WG)
    step2(WKV)
    step1(WQ)
    step3(WKV)
    step2(WG)
    step2(WQ)
    step4(WKV)
    for c in range(2):
        part = dot(normed[pl.ds(c * half, half)], wkv[...])
        keys_t = jnp.transpose(part[:, :128]).astype(BF16)
        kv[me * 2 + c, pl.ds(0, 128)] = keys_t[:, :128]
        kv[me * 2 + c, pl.ds(128, 128)] = keys_t[:, 128:]
        kv[me * 2 + c, pl.ds(256, 256)] = part[:, 128:].astype(BF16)
    step3(WG)
    step3(WQ)
    step0(KV)
    step4(WG)
    planes_start()
    step4(WQ)
    for c in range(2):
        at = pl.ds(c * half, half)
        q[at] = dot(normed[at], wq[...]).astype(BF16)
    for c in range(2):
        attend_own(c)
    step1(KV)
    loads[6].wait()
    step0(WOA)
    attend_group(0, 2, straight)
    loads[7].wait()
    step0(WOB)
    attend_group(2, 2, straight)
    step2(KV)
    attend_group(0, 2, corner)
    planes_forward(0)
    planes_forward(1)
    step1(WOA)
    attend_group(2, 2, corner)
    step1(WOB)
    planes_forward(2)
    planes_forward(3)
    attend_group(0, 2, opposite)
    step3(KV)
    attend_group(0, 2, knight)
    for b in range(4):
        for w in range(2):
            plane_message(b, w, True, True).wait_recv()
    step2(WOB)
    step2(WOA)
    lax.fori_loop(0, rows // 256, gate_rows, 0)
    for k in range(4):
        rim_box[0, k] = gpad[k, pl.ds(rows, 32)].astype(BF16)
    rim.start()
    attend_group(2, 2, knight)
    step4(KV)
    rim.wait_recv()
    step3(WOB)
    inside = jnp.where(me > 0, 1.0, 0.0)
    for k in range(4):
        gpad[k, pl.ds(0, 32)] = rim_box[1, k].astype(F32) * inside

    lax.fori_loop(0, rows // 64, conv_rows_of, 0)
    sq.start()
    attend_group(0, 1, lambda i: (2, 2))
    step3(WOA)
    lax.fori_loop(0, rows // 128, finish_rows, 0)
    sq.wait_recv()
    lax.fori_loop(0, rows // 64, act_rows, 0)
    step4(WOB)
    step4(WOA)
    for n in range(2):
        outbox[n] = dot(both[theirs], out_columns(n)).astype(BF16)
        out_copy(n).start()
    for n in range(2):
        part = dot(both[ours], out_columns(n))
        out_copy(n).wait_recv()
        mixed_ref[:, pl.ds(n * 1024, 1024)] = (part + inbox[n].astype(F32)).astype(BF16)

    for job in range(6):
        for c, w in BOTH:
            for kind in KINDS:
                message(job, c, w, kind).wait_send()
    for b in range(4):
        for w in range(2):
            plane_message(b, w, False).wait_send()
            plane_message(b, w, True).wait_send()
    rim.wait_send()
    sq.wait_send()

    for n in range(2):
        out_copy(n).wait_send()


def body(
    tokens, norm_gain, w_query, w_key, w_value, w_glu_value, w_glu_gate, conv_taps, convolution_norm_gain, head_gain, lam, w_out,
):
    rows = tokens.shape[0]
    d = tokens.shape[1]
    vmem = pl.BlockSpec(memory_space=pltpu.VMEM)
    smem = pl.BlockSpec(memory_space=pltpu.SMEM)
    dma = pltpu.SemaphoreType.DMA
    mixed, logs = pl.pallas_call(
        kernel,
        out_shape=(jax.ShapeDtypeStruct((rows // 2, d), BF16), jax.ShapeDtypeStruct((8, rows), F32)),
        in_specs=[ANY, vmem, ANY, ANY, ANY, ANY, ANY, vmem, vmem, vmem, smem, ANY],
        out_specs=(vmem, vmem),
        scratch_shapes=[
            pltpu.VMEM((rows, d), BF16),
            pltpu.VMEM((rows, d), BF16),
            pltpu.VMEM((d, 256), BF16),
            pltpu.VMEM((d, 512), BF16),
            pltpu.VMEM((4, 2, d, 128), BF16),
            pltpu.VMEM((RING, 1024, 128), BF16),
            pltpu.VMEM((2 * RING, 512, 128), BF16),
            pltpu.VMEM((rows, 512), BF16),
            pltpu.VMEM((8, rows, 128), F32),
            pltpu.VMEM((8, rows, 128), F32),
            pltpu.VMEM((4, rows + 32, 128), F32),
            pltpu.VMEM((rows, 512), F32),
            pltpu.VMEM((rows, 128), F32),
            pltpu.VMEM((rows, 1024), BF16),
            pltpu.VMEM((2, 256, 1024), BF16),
            pltpu.VMEM((2, 256, 1024), BF16),
            pltpu.VMEM((2, 4, 32, 128), BF16),
            pltpu.VMEM((rows, 128), F32),
            pltpu.VMEM((31, 512), F32),
            dma((8,)),
            dma((6, 2, 2, len(KINDS))),
            dma((6, 2, 2, len(KINDS))),
            dma((16,)),
            dma((16,)),
            dma((2,)),
            dma((2,)),
            dma((2,)),
            dma((2,)),
        ],
        compiler_params=pltpu.CompilerParams(
            collective_id=0, has_side_effects=True, vmem_limit_bytes=60 * 1024 * 1024
        ),
    )(
        tokens, norm_gain, w_query, w_key, w_value, w_glu_value, w_glu_gate,
        conv_taps, convolution_norm_gain, head_gain.reshape(1, -1), lam, w_out,
    )
    return mixed, logs.T


def solution(mesh):
    return jax.shard_map(
        body,
        mesh=mesh,
        in_specs=(
            P(("fs", "sp"), None),
            P(),
            P("sp", "tp"),
            P("sp", "tp"),
            P("sp", "tp"),
            P("sp", "tp"),
            P("sp", "tp"),
            P(None, "tp"),
            P(),
            P(),
            P("tp"),
            P(None, "sp"),
        ),
        out_specs=(P(("fs", "sp", "tp"), None), P(("fs", "sp"), "tp")),
        check_vma=False,
    )
```

```python
import functools
import math

import jax
import jax.numpy as jnp
from jax import lax
from jax.experimental import pallas as pl
from jax.experimental.pallas import tpu as pltpu
from jax.sharding import PartitionSpec as P

HEADS = 8
QK = 64
VDIM = 128
CONV = 1024
EPS = 1e-06
RING = 16
MESH = pl.DeviceIdType.MESH
ANY = pl.BlockSpec(memory_space=pl.ANY)
F32 = jnp.float32
BF16 = jnp.bfloat16


def dot(a, b):
    return jnp.dot(a, b, preferred_element_type=F32)


KINDS = ("u1", "u2", "v0", "vm", "vp", "q0", "q1", "f0", "fm", "fp", "f2")
WAYS = ((0, 1), (1, -1))


def kernel(
    tok_hbm, ngain_ref, wq_hbm, wk_hbm, wv_hbm, wgv_hbm, wgg_hbm, taps_ref, cgain_ref, hgain_ref, lam_ref, wout_hbm,
    mixed_ref, logt_ref,
    tok, normed, wkv, wq, wg, wo, kv, q, acc, lsum, gpad, conv, squares, both, outbox, inbox, rim_box, sq_in, taps,
    load_sem, send_sem, recv_sem, plane_send, plane_recv, side_send, side_recv, out_send, out_recv,
):
    rows = tok.shape[0]
    me = lax.axis_index("sp")
    core = lax.axis_index("tp")
    plane = lax.axis_index("fs")
    mine_z, mine_x = lax.div(me, 4), lax.rem(me, 4)
    after, before = lax.rem(me + 1, RING), lax.rem(me + RING - 1, RING)
    planes = [lax.rem(plane + 1, 4), lax.rem(plane + 3, 4)]

    def at_offset(dx, dz):
        return lax.rem(mine_z + dz + 8, 4) * 4 + lax.rem(mine_x + dx + 8, 4)

    def offset(c, du, dv):
        return at_offset(du, dv) if c == 0 else at_offset(dv, du)

    mine = pl.ds(pl.multiple_of(me * 128, 128), 128)
    quarter = pl.ds(pl.multiple_of(plane * 128, 128), 128)
    att_rows = pl.ds(pl.multiple_of(core * 512, 512), 512)
    conv_rows = pl.ds(pl.multiple_of(1024 + core * 512, 512), 512)
    loads = [
        (wk_hbm, wkv.at[mine, pl.ds(0, 128)]),
        (wv_hbm, wkv.at[mine, pl.ds(128, 128)]),
        (wq_hbm, wq.at[mine]),
        (wgv_hbm.at[:, quarter], wg.at[plane, 0, mine]),
        (wgg_hbm.at[:, quarter], wg.at[plane, 1, mine]),
        (tok_hbm, tok),
        (wout_hbm.at[att_rows], wo.at[me, pl.ds(0, 512)]),
        (wout_hbm.at[conv_rows], wo.at[me, pl.ds(512, 512)]),
    ]
    loads = [pltpu.make_async_copy(s, d, load_sem.at[i]) for i, (s, d) in enumerate(loads)]
    for load in loads:
        load.start()

    barrier = pltpu.get_barrier_semaphore()
    for peer in [offset(c, s, 0) for c in range(2) for _, s in WAYS] + [after, before]:
        pl.semaphore_signal(barrier, inc=1, device_id={"sp": peer}, device_id_type=MESH)
    for peer in planes:
        pl.semaphore_signal(barrier, inc=1, device_id={"fs": peer}, device_id_type=MESH)
    pl.semaphore_signal(barrier, inc=1, device_id={"tp": 1 - core}, device_id_type=MESH)
    pl.semaphore_wait(barrier, 9)

    def weight_rows(ref):
        def part(source, c, at, size):
            start = source * 128 + c * 64 + at * 32
            return ref.at[pl.ds(pl.multiple_of(start, 32), size * 32)]
        return part

    def glu_rows(source, c, at, size):
        start = source * 128 + c * 64 + at * 32
        return wg.at[plane, :, pl.ds(pl.multiple_of(start, 32), size * 32)]

    def out_rows(first):
        def part(source, c, at, size):
            return wo.at[source, pl.ds(first + c * 256 + at * 128, size * 128)]
        return part

    def kv_rows(source, c, at, size):
        return kv.at[source * 2 + c, pl.ds(at * 256, size * 256)]

    jobs = [weight_rows(wkv), weight_rows(wq), glu_rows, kv_rows, out_rows(0), out_rows(512)]
    WKV, WQ, WG, KV, WOA, WOB = range(6)

    def message(job, c, w, kind, arriving=False):
        sign = WAYS[w][1]
        along = kind[0] == "u"
        du = {"u1": 0, "u2": -sign, "v0": 0, "f0": 0, "vm": -1, "fm": -1, "vp": 1, "fp": 1, "q0": 2, "q1": 2, "f2": 2}[kind]
        dv = -sign if kind[0] == "f" else 0
        at, size = {"u1": (0, 2), "v0": (0, 2), "vm": (0, 2), "vp": (0, 2), "q0": (0, 1), "q1": (1, 1)}.get(kind, (w, 1))
        peer = offset(c, sign, 0) if along else offset(c, 0, sign)
        if arriving:
            du, dv = (du - sign, dv) if along else (du, dv - sign)
        ref = jobs[job](offset(c, du, dv), c, at, size)
        k = KINDS.index(kind)
        return pltpu.make_async_remote_copy(
            src_ref=ref, dst_ref=ref, send_sem=send_sem.at[job, c, w, k], recv_sem=recv_sem.at[job, c, w, k],
            device_id={"sp": peer}, device_id_type=MESH,
        )

    def go(job, c, w, kind):
        message(job, c, w, kind).start()

    def come(job, c, w, kind):
        message(job, c, w, kind, True).wait_recv()

    BOTH = ((0, 0), (0, 1), (1, 0), (1, 1))

    def step0(job):
        for c, w in BOTH:
            go(job, c, w, "u1")
        for c, w in BOTH:
            go(job, c, w, "v0")

    def step1(job):
        for c, w in BOTH:
            come(job, c, w, "u1")
            go(job, c, w, "u2")
            for w2 in range(2):
                go(job, c, w2, "vm" if w == 0 else "vp")
        for c, w in BOTH:
            come(job, c, w, "v0")
            go(job, c, w, "f0")

    def step2(job):
        for c, w in BOTH:
            come(job, c, w, "u2")
            for w2 in range(2):
                go(job, c, w2, "q0" if w == 0 else "q1")
        for c, w in BOTH:
            for side in "mp":
                come(job, c, w, "v" + side)
                go(job, c, w, "f" + side)
        for c, w in BOTH:
            come(job, c, w, "f0")

    def step3(job):
        for c, w in BOTH:
            come(job, c, w, "q0")
            come(job, c, w, "q1")
            go(job, c, w, "f2")
        for c, w in BOTH:
            come(job, c, w, "fm")
            come(job, c, w, "fp")

    def step4(job):
        for c, w in BOTH:
            come(job, c, w, "f2")

    def plane_message(b, w, forward, arriving=False):
        sign = WAYS[w][1]
        back = (1 if forward else 0) + (1 if arriving else 0)
        owner = lax.rem(plane - sign * back + 8, 4)
        start = b * 512 + (w * 256 if forward else 0)
        ref = wg.at[owner, :, pl.ds(start, 256 if forward else 512)]
        k = 4 * b + 2 * w + (1 if forward else 0)
        return pltpu.make_async_remote_copy(
            src_ref=ref, dst_ref=ref, send_sem=plane_send.at[k], recv_sem=plane_recv.at[k],
            device_id={"fs": planes[w]}, device_id_type=MESH,
        )

    def planes_start():
        for b in range(4):
            for w in range(2):
                plane_message(b, w, False).start()

    def planes_forward(b):
        for w in range(2):
            plane_message(b, w, False, True).wait_recv()
            plane_message(b, w, True).start()

    half = rows // 2

    def norm_rows(i, carry):
        at = pl.ds(pl.multiple_of(i * 64, 64), 64)
        t = tok[at].astype(F32)
        scale = lax.rsqrt(jnp.mean(t * t, axis=-1, keepdims=True) + EPS)
        normed[at] = (t * scale * ngain_ref[...].astype(F32).reshape(1, -1)).astype(BF16)
        return carry

    c_exp = QK ** (-0.5) * math.log2(math.e)

    def keys_of(pieces, m):
        parts = []
        for piece in pieces:
            k = kv[piece, pl.ds(0, 256)]
            parts += [k[:128], k[128:]]
        wide = jnp.concatenate(parts, axis=1)
        zero = jnp.zeros((QK, wide.shape[1]), BF16)
        return jnp.concatenate([wide[:QK], zero] if m == 0 else [zero, wide[QK:]], axis=0)

    def lane_sum(w):
        s = w[:, :128]
        for k in range(1, w.shape[1] // 128):
            s = s + w[:, k * 128 : k * 128 + 128]
        return s

    def attend_source(source):
        pieces = [source * 2, source * 2 + 1]
        values = jnp.concatenate([kv[p, pl.ds(256, 256)] for p in pieces], axis=0)
        keys = [keys_of(pieces, m) for m in range(2)]
        for h in range(4):
            queries = q[:, pl.ds(h * 128, 128)]
            for m in range(2):
                w = jnp.exp2(dot(queries, keys[m]) * c_exp)
                s = lane_sum(w)
                o = dot(w.astype(BF16), values)
                lsum[h * 2 + m] += s
                acc[h * 2 + m] += o

    def attend_own(c):
        start = c * half
        pieces = [me * 2, me * 2 + 1][: c + 1]
        values = jnp.concatenate([kv[p, pl.ds(256, 256)] for p in pieces], axis=0)
        keys = [keys_of(pieces, m) for m in range(2)]
        at = pl.ds(start, half)
        width = 256 * len(pieces)
        key_pos = lax.broadcasted_iota(jnp.int32, (half, width), 1)
        row_pos = start + lax.broadcasted_iota(jnp.int32, (half, width), 0)
        for h in range(4):
            queries = q[at, pl.ds(h * 128, 128)]
            for m in range(2):
                w = jnp.exp2(dot(queries, keys[m]) * c_exp)
                w = jnp.where(key_pos <= row_pos, w, 0.0)
                lsum[h * 2 + m, at] = lane_sum(w)
                acc[h * 2 + m, at] = dot(w.astype(BF16), values)

    def attend_group(first, count, where):
        def one(i, carry):
            dx, dz = where(i)
            source = at_offset(dx, dz)

            @pl.when(source < me)
            def _():
                attend_source(source)
            return carry

        lax.fori_loop(first, first + count, one, 0)

    def odd(i):
        return 1 + 2 * lax.rem(i, 2)

    def straight(i):
        return (1 - lax.div(i, 2)) * odd(i), lax.div(i, 2) * odd(i)

    def corner(i):
        return 1 + 2 * lax.div(i, 2), odd(i)

    def opposite(i):
        return 2 * (1 - i), 2 * i

    def knight(i):
        side = lax.div(i, 2)
        return 2 * (1 - side) + side * odd(i), 2 * side + (1 - side) * odd(i)

    def gate_rows():
        value = dot(normed[...], jnp.concatenate([wg[k, 0] for k in range(4)], axis=1))
        gate = dot(normed[...], jnp.concatenate([wg[k, 1] for k in range(4)], axis=1))
        gated = (value * jax.nn.sigmoid(gate)).astype(BF16).astype(F32)
        for k in range(4):
            gpad[k, pl.ds(32, rows)] = gated[:, k * 128 : k * 128 + 128]

    rim = pltpu.make_async_remote_copy(
        src_ref=rim_box.at[0], dst_ref=rim_box.at[1], send_sem=side_send.at[0], recv_sem=side_recv.at[0],
        device_id={"sp": after}, device_id_type=MESH,
    )

    def finish_rows(i, carry):
        at = pl.ds(pl.multiple_of(i * 128, 128), 128)
        lane = lax.broadcasted_iota(jnp.int32, (128, 128), 1)
        logs = jnp.zeros((128, 128), F32)
        for h in range(4):
            t0 = jnp.sum(lsum[2 * h, at], axis=-1, keepdims=True)
            t1 = jnp.sum(lsum[2 * h + 1, at], axis=-1, keepdims=True)
            diff = acc[2 * h, at] / t0 - lam_ref[h] * acc[2 * h + 1, at] / t1
            out = diff * lax.rsqrt(jnp.mean(diff * diff, axis=-1, keepdims=True) + EPS) * hgain_ref[...].astype(F32)
            both[at, pl.ds(h * 128, 128)] = out.astype(BF16)
            logs = jnp.where(lane == 2 * h, t0, logs)
            logs = jnp.where(lane == 2 * h + 1, t1, logs)
        logt_ref[:, at] = jnp.log(jnp.transpose(logs)[:8])
        return carry


    def conv_rows_of(i, carry):
        base = pl.multiple_of(i * 64, 64)
        total = jnp.zeros((64, 128), F32)
        for k in range(4):
            out = jnp.zeros((64, 128), F32)
            for j in range(31):
                out = out + taps[pl.ds(j, 1), pl.ds(k * 128, 128)] * gpad[k, pl.ds(base + (j + 2), 64)]
            out = out.astype(BF16).astype(F32)
            conv[pl.ds(base, 64), pl.ds(k * 128, 128)] = out
            total = total + out * out
        squares[pl.ds(base, 64)] = total
        return carry

    sq = pltpu.make_async_remote_copy(
        src_ref=squares, dst_ref=sq_in, send_sem=side_send.at[1], recv_sem=side_recv.at[1],
        device_id={"tp": 1 - core}, device_id_type=MESH,
    )

    def act_rows(i, carry):
        at = pl.ds(pl.multiple_of(i * 128, 128), 128)
        total = jnp.sum(squares[at] + sq_in[at], axis=-1, keepdims=True)
        gain = cgain_ref[pl.ds(pl.multiple_of(core * 512, 512), 512)].astype(F32).reshape(1, 512)
        x = conv[at] * lax.rsqrt(total / CONV + EPS) * gain
        both[at, pl.ds(512, 512)] = (x * jax.nn.sigmoid(x)).astype(BF16)
        return carry

    def out_copy(n):
        return pltpu.make_async_remote_copy(
            src_ref=outbox.at[n], dst_ref=inbox.at[n], send_sem=out_send.at[n], recv_sem=out_recv.at[n],
            device_id={"tp": 1 - core}, device_id_type=MESH,
        )

    theirs = pl.ds(pl.multiple_of((1 - core) * 256, 256), 256)
    ours = pl.ds(pl.multiple_of(core * 256, 256), 256)

    def out_columns(n):
        return jnp.concatenate([wo[8 * n + k] for k in range(8)], axis=1)

    loads[3].wait()
    loads[4].wait()
    step0(WG)
    loads[2].wait()
    step0(WQ)
    loads[0].wait()
    loads[1].wait()
    step0(WKV)
    step1(WG)
    step1(WKV)
    step2(WG)
    step2(WKV)
    step1(WQ)
    step3(WG)
    step3(WKV)
    loads[5].wait()
    lax.fori_loop(0, rows // 64, norm_rows, 0)
    taps[...] = taps_ref[...].astype(F32)
    step2(WQ)
    step4(WKV)
    for c in range(2):
        part = dot(normed[pl.ds(c * half, half)], wkv[...])
        keys_t = jnp.transpose(part[:, :128]).astype(BF16)
        kv[me * 2 + c, pl.ds(0, 128)] = keys_t[:, :128]
        kv[me * 2 + c, pl.ds(128, 128)] = keys_t[:, 128:]
        kv[me * 2 + c, pl.ds(256, 256)] = part[:, 128:].astype(BF16)
    step4(WG)
    planes_start()
    step3(WQ)
    step0(KV)
    step4(WQ)
    for c in range(2):
        at = pl.ds(c * half, half)
        q[at] = dot(normed[at], wq[...]).astype(BF16)
    for c in range(2):
        attend_own(c)
    step1(KV)
    attend_group(0, 2, straight)
    planes_forward(0)
    planes_forward(1)
    loads[7].wait()
    step0(WOB)
    loads[6].wait()
    step0(WOA)
    attend_group(2, 2, straight)
    step2(KV)
    attend_group(0, 2, corner)
    attend_group(2, 2, corner)
    step1(WOA)
    step1(WOB)
    planes_forward(2)
    planes_forward(3)
    attend_group(0, 2, opposite)
    step3(KV)
    attend_group(0, 2, knight)
    for b in range(4):
        for w in range(2):
            plane_message(b, w, True, True).wait_recv()
    step2(WOA)
    gate_rows()
    for k in range(4):
        rim_box[0, k] = gpad[k, pl.ds(rows, 32)].astype(BF16)
    rim.start()
    step2(WOB)
    attend_group(2, 2, knight)
    rim.wait_recv()
    inside = jnp.where(me > 0, 1.0, 0.0)
    for k in range(4):
        gpad[k, pl.ds(0, 32)] = rim_box[1, k].astype(F32) * inside

    lax.fori_loop(0, rows // 64, conv_rows_of, 0)
    sq.start()
    step4(KV)
    step3(WOB)
    step3(WOA)
    attend_group(0, 1, lambda i: (2, 2))
    lax.fori_loop(0, rows // 128, finish_rows, 0)
    sq.wait_recv()
    step4(WOB)
    lax.fori_loop(0, rows // 128, act_rows, 0)
    step4(WOA)
    for n in range(2):
        outbox[n] = dot(both[theirs], out_columns(n)).astype(BF16)
        out_copy(n).start()
    for n in range(2):
        part = dot(both[ours], out_columns(n))
        out_copy(n).wait_recv()
        mixed_ref[:, pl.ds(n * 1024, 1024)] = (part + inbox[n].astype(F32)).astype(BF16)

    for job in range(6):
        for c, w in BOTH:
            for kind in KINDS:
                message(job, c, w, kind).wait_send()
    for b in range(4):
        for w in range(2):
            plane_message(b, w, False).wait_send()
            plane_message(b, w, True).wait_send()
    rim.wait_send()
    sq.wait_send()

    for n in range(2):
        out_copy(n).wait_send()


def body(
    tokens, norm_gain, w_query, w_key, w_value, w_glu_value, w_glu_gate, conv_taps, convolution_norm_gain, head_gain, lam, w_out,
):
    rows = tokens.shape[0]
    d = tokens.shape[1]
    vmem = pl.BlockSpec(memory_space=pltpu.VMEM)
    smem = pl.BlockSpec(memory_space=pltpu.SMEM)
    dma = pltpu.SemaphoreType.DMA
    mixed, logs = pl.pallas_call(
        kernel,
        out_shape=(jax.ShapeDtypeStruct((rows // 2, d), BF16), jax.ShapeDtypeStruct((8, rows), F32)),
        in_specs=[ANY, vmem, ANY, ANY, ANY, ANY, ANY, vmem, vmem, vmem, smem, ANY],
        out_specs=(vmem, vmem),
        scratch_shapes=[
            pltpu.VMEM((rows, d), BF16),
            pltpu.VMEM((rows, d), BF16),
            pltpu.VMEM((d, 256), BF16),
            pltpu.VMEM((d, 512), BF16),
            pltpu.VMEM((4, 2, d, 128), BF16),
            pltpu.VMEM((RING, 1024, 128), BF16),
            pltpu.VMEM((2 * RING, 512, 128), BF16),
            pltpu.VMEM((rows, 512), BF16),
            pltpu.VMEM((8, rows, 128), F32),
            pltpu.VMEM((8, rows, 128), F32),
            pltpu.VMEM((4, rows + 32, 128), F32),
            pltpu.VMEM((rows, 512), F32),
            pltpu.VMEM((rows, 128), F32),
            pltpu.VMEM((rows, 1024), BF16),
            pltpu.VMEM((2, 256, 1024), BF16),
            pltpu.VMEM((2, 256, 1024), BF16),
            pltpu.VMEM((2, 4, 32, 128), BF16),
            pltpu.VMEM((rows, 128), F32),
            pltpu.VMEM((31, 512), F32),
            dma((8,)),
            dma((6, 2, 2, len(KINDS))),
            dma((6, 2, 2, len(KINDS))),
            dma((16,)),
            dma((16,)),
            dma((2,)),
            dma((2,)),
            dma((2,)),
            dma((2,)),
        ],
        compiler_params=pltpu.CompilerParams(
            collective_id=0, has_side_effects=True, vmem_limit_bytes=60 * 1024 * 1024
        ),
    )(
        tokens, norm_gain, w_query, w_key, w_value, w_glu_value, w_glu_gate,
        conv_taps, convolution_norm_gain, head_gain.reshape(1, -1), lam, w_out,
    )
    return mixed, logs.T


def solution(mesh):
    return jax.shard_map(
        body,
        mesh=mesh,
        in_specs=(
            P(("fs", "sp"), None),
            P(),
            P("sp", "tp"),
            P("sp", "tp"),
            P("sp", "tp"),
            P("sp", "tp"),
            P("sp", "tp"),
            P(None, "tp"),
            P(),
            P(),
            P("tp"),
            P(None, "sp"),
        ),
        out_specs=(P(("fs", "sp", "tp"), None), P(("fs", "sp"), "tp")),
        check_vma=False,
    )
```

```python
import functools
import math

import jax
import jax.numpy as jnp
from jax import lax
from jax.experimental import pallas as pl
from jax.experimental.pallas import tpu as pltpu
from jax.sharding import PartitionSpec as P

HEADS = 8
QK = 64
VDIM = 128
CONV = 1024
EPS = 1e-06
RING = 16
MESH = pl.DeviceIdType.MESH
ANY = pl.BlockSpec(memory_space=pl.ANY)
F32 = jnp.float32
BF16 = jnp.bfloat16


def dot(a, b):
    return jnp.dot(a, b, preferred_element_type=F32)


KINDS = ("u1", "u2", "v0", "vm", "vp", "q0", "q1", "f0", "fm", "fp", "f2")
WAYS = ((0, 1), (1, -1))


def kernel(
    tok_hbm, ngain_ref, wq_hbm, wk_hbm, wv_hbm, wgv_hbm, wgg_hbm, taps_ref, cgain_ref, hgain_ref, lam_ref, wout_hbm,
    mixed_ref, logt_ref,
    tok, normed, wkv, wq, wg, wo, kv, q, acc, lsum, gpad, conv, squares, both, outbox, inbox, rim_box, sq_in, taps,
    load_sem, send_sem, recv_sem, plane_send, plane_recv, side_send, side_recv, out_send, out_recv,
):
    rows = tok.shape[0]
    me = lax.axis_index("sp")
    core = lax.axis_index("tp")
    plane = lax.axis_index("fs")
    mine_z, mine_x = lax.div(me, 4), lax.rem(me, 4)
    after, before = lax.rem(me + 1, RING), lax.rem(me + RING - 1, RING)
    planes = [lax.rem(plane + 1, 4), lax.rem(plane + 3, 4)]

    def at_offset(dx, dz):
        return lax.rem(mine_z + dz + 8, 4) * 4 + lax.rem(mine_x + dx + 8, 4)

    def offset(c, du, dv):
        return at_offset(du, dv) if c == 0 else at_offset(dv, du)

    mine = pl.ds(pl.multiple_of(me * 128, 128), 128)
    quarter = pl.ds(pl.multiple_of(plane * 128, 128), 128)
    att_rows = pl.ds(pl.multiple_of(core * 512, 512), 512)
    conv_rows = pl.ds(pl.multiple_of(1024 + core * 512, 512), 512)
    loads = [
        (wk_hbm, wkv.at[mine, pl.ds(0, 128)]),
        (wv_hbm, wkv.at[mine, pl.ds(128, 128)]),
        (wq_hbm, wq.at[mine]),
        (wgv_hbm.at[:, quarter], wg.at[plane, 0, mine]),
        (wgg_hbm.at[:, quarter], wg.at[plane, 1, mine]),
        (tok_hbm, tok),
        (wout_hbm.at[att_rows], wo.at[me, pl.ds(0, 512)]),
        (wout_hbm.at[conv_rows], wo.at[me, pl.ds(512, 512)]),
    ]
    loads = [pltpu.make_async_copy(s, d, load_sem.at[i]) for i, (s, d) in enumerate(loads)]
    for load in loads:
        load.start()

    barrier = pltpu.get_barrier_semaphore()
    for peer in [offset(c, s, 0) for c in range(2) for _, s in WAYS] + [after, before]:
        pl.semaphore_signal(barrier, inc=1, device_id={"sp": peer}, device_id_type=MESH)
    for peer in planes:
        pl.semaphore_signal(barrier, inc=1, device_id={"fs": peer}, device_id_type=MESH)
    pl.semaphore_signal(barrier, inc=1, device_id={"tp": 1 - core}, device_id_type=MESH)
    pl.semaphore_wait(barrier, 9)

    def weight_rows(ref):
        def part(source, c, at, size):
            start = source * 128 + c * 64 + at * 32
            return ref.at[pl.ds(pl.multiple_of(start, 32), size * 32)]
        return part

    def glu_rows(source, c, at, size):
        start = source * 128 + c * 64 + at * 32
        return wg.at[plane, :, pl.ds(pl.multiple_of(start, 32), size * 32)]

    def out_rows(first):
        def part(source, c, at, size):
            return wo.at[source, pl.ds(first + c * 256 + at * 128, size * 128)]
        return part

    def kv_rows(source, c, at, size):
        return kv.at[source * 2 + c, pl.ds(at * 256, size * 256)]

    jobs = [weight_rows(wkv), weight_rows(wq), glu_rows, kv_rows, out_rows(0), out_rows(512)]
    WKV, WQ, WG, KV, WOA, WOB = range(6)

    def message(job, c, w, kind, arriving=False):
        sign = WAYS[w][1]
        along = kind[0] == "u"
        du = {"u1": 0, "u2": -sign, "v0": 0, "f0": 0, "vm": -1, "fm": -1, "vp": 1, "fp": 1, "q0": 2, "q1": 2, "f2": 2}[kind]
        dv = -sign if kind[0] == "f" else 0
        at, size = {"u1": (0, 2), "v0": (0, 2), "vm": (0, 2), "vp": (0, 2), "q0": (0, 1), "q1": (1, 1)}.get(kind, (w, 1))
        peer = offset(c, sign, 0) if along else offset(c, 0, sign)
        if arriving:
            du, dv = (du - sign, dv) if along else (du, dv - sign)
        ref = jobs[job](offset(c, du, dv), c, at, size)
        k = KINDS.index(kind)
        return pltpu.make_async_remote_copy(
            src_ref=ref, dst_ref=ref, send_sem=send_sem.at[job, c, w, k], recv_sem=recv_sem.at[job, c, w, k],
            device_id={"sp": peer}, device_id_type=MESH,
        )

    def go(job, c, w, kind):
        message(job, c, w, kind).start()

    def come(job, c, w, kind):
        message(job, c, w, kind, True).wait_recv()

    BOTH = ((0, 0), (0, 1), (1, 0), (1, 1))

    def step0(job):
        for c, w in BOTH:
            go(job, c, w, "u1")
        for c, w in BOTH:
            go(job, c, w, "v0")

    def step1(job):
        for c, w in BOTH:
            come(job, c, w, "u1")
            go(job, c, w, "u2")
            for w2 in range(2):
                go(job, c, w2, "vm" if w == 0 else "vp")
        for c, w in BOTH:
            come(job, c, w, "v0")
            go(job, c, w, "f0")

    def step2(job):
        for c, w in BOTH:
            come(job, c, w, "u2")
            for w2 in range(2):
                go(job, c, w2, "q0" if w == 0 else "q1")
        for c, w in BOTH:
            for side in "mp":
                come(job, c, w, "v" + side)
                go(job, c, w, "f" + side)
        for c, w in BOTH:
            come(job, c, w, "f0")

    def step3(job):
        for c, w in BOTH:
            come(job, c, w, "q0")
            come(job, c, w, "q1")
            go(job, c, w, "f2")
        for c, w in BOTH:
            come(job, c, w, "fm")
            come(job, c, w, "fp")

    def step4(job):
        for c, w in BOTH:
            come(job, c, w, "f2")

    def plane_message(b, w, forward, arriving=False):
        sign = WAYS[w][1]
        back = (1 if forward else 0) + (1 if arriving else 0)
        owner = lax.rem(plane - sign * back + 8, 4)
        start = b * 512 + (w * 256 if forward else 0)
        ref = wg.at[owner, :, pl.ds(start, 256 if forward else 512)]
        k = 4 * b + 2 * w + (1 if forward else 0)
        return pltpu.make_async_remote_copy(
            src_ref=ref, dst_ref=ref, send_sem=plane_send.at[k], recv_sem=plane_recv.at[k],
            device_id={"fs": planes[w]}, device_id_type=MESH,
        )

    def planes_start():
        for b in range(4):
            for w in range(2):
                plane_message(b, w, False).start()

    def planes_forward(b):
        for w in range(2):
            plane_message(b, w, False, True).wait_recv()
            plane_message(b, w, True).start()

    half = rows // 2

    def norm_rows(i, carry):
        at = pl.ds(pl.multiple_of(i * 64, 64), 64)
        t = tok[at].astype(F32)
        scale = lax.rsqrt(jnp.mean(t * t, axis=-1, keepdims=True) + EPS)
        normed[at] = (t * scale * ngain_ref[...].astype(F32).reshape(1, -1)).astype(BF16)
        return carry

    c_exp = QK ** (-0.5) * math.log2(math.e)

    def keys_of(pieces, m):
        parts = []
        for piece in pieces:
            k = kv[piece, pl.ds(0, 256)]
            parts += [k[:128], k[128:]]
        wide = jnp.concatenate(parts, axis=1)
        zero = jnp.zeros((QK, wide.shape[1]), BF16)
        return jnp.concatenate([wide[:QK], zero] if m == 0 else [zero, wide[QK:]], axis=0)

    def lane_sum(w):
        s = w[:, :128]
        for k in range(1, w.shape[1] // 128):
            s = s + w[:, k * 128 : k * 128 + 128]
        return s

    def attend_source(source):
        pieces = [source * 2, source * 2 + 1]
        values = jnp.concatenate([kv[p, pl.ds(256, 256)] for p in pieces], axis=0)
        keys = [keys_of(pieces, m) for m in range(2)]
        for h in range(4):
            queries = q[:, pl.ds(h * 128, 128)]
            for m in range(2):
                w = jnp.exp2(dot(queries, keys[m]) * c_exp)
                s = lane_sum(w)
                o = dot(w.astype(BF16), values)
                lsum[h * 2 + m] += s
                acc[h * 2 + m] += o

    def attend_own(c):
        start = c * half
        pieces = [me * 2, me * 2 + 1][: c + 1]
        values = jnp.concatenate([kv[p, pl.ds(256, 256)] for p in pieces], axis=0)
        keys = [keys_of(pieces, m) for m in range(2)]
        at = pl.ds(start, half)
        width = 256 * len(pieces)
        key_pos = lax.broadcasted_iota(jnp.int32, (half, width), 1)
        row_pos = start + lax.broadcasted_iota(jnp.int32, (half, width), 0)
        for h in range(4):
            queries = q[at, pl.ds(h * 128, 128)]
            for m in range(2):
                w = jnp.exp2(dot(queries, keys[m]) * c_exp)
                w = jnp.where(key_pos <= row_pos, w, 0.0)
                lsum[h * 2 + m, at] = lane_sum(w)
                acc[h * 2 + m, at] = dot(w.astype(BF16), values)

    def attend_group(first, count, where):
        def one(i, carry):
            dx, dz = where(i)
            source = at_offset(dx, dz)

            @pl.when(source < me)
            def _():
                attend_source(source)
            return carry

        lax.fori_loop(first, first + count, one, 0)

    def odd(i):
        return 1 + 2 * lax.rem(i, 2)

    def straight(i):
        return (1 - lax.div(i, 2)) * odd(i), lax.div(i, 2) * odd(i)

    def corner(i):
        return 1 + 2 * lax.div(i, 2), odd(i)

    def opposite(i):
        return 2 * (1 - i), 2 * i

    def knight(i):
        side = lax.div(i, 2)
        return 2 * (1 - side) + side * odd(i), 2 * side + (1 - side) * odd(i)

    def gate_rows():
        value = dot(normed[...], jnp.concatenate([wg[k, 0] for k in range(4)], axis=1))
        gate = dot(normed[...], jnp.concatenate([wg[k, 1] for k in range(4)], axis=1))
        gated = (value * jax.nn.sigmoid(gate)).astype(BF16).astype(F32)
        for k in range(4):
            gpad[k, pl.ds(32, rows)] = gated[:, k * 128 : k * 128 + 128]

    rim = pltpu.make_async_remote_copy(
        src_ref=rim_box.at[0], dst_ref=rim_box.at[1], send_sem=side_send.at[0], recv_sem=side_recv.at[0],
        device_id={"sp": after}, device_id_type=MESH,
    )

    def finish_rows(i, carry):
        at = pl.ds(pl.multiple_of(i * 256, 256), 256)
        lane = lax.broadcasted_iota(jnp.int32, (256, 128), 1)
        logs = jnp.zeros((256, 128), F32)
        for h in range(4):
            t0 = jnp.sum(lsum[2 * h, at], axis=-1, keepdims=True)
            t1 = jnp.sum(lsum[2 * h + 1, at], axis=-1, keepdims=True)
            diff = acc[2 * h, at] / t0 - lam_ref[h] * acc[2 * h + 1, at] / t1
            out = diff * lax.rsqrt(jnp.mean(diff * diff, axis=-1, keepdims=True) + EPS) * hgain_ref[...].astype(F32)
            both[at, pl.ds(h * 128, 128)] = out.astype(BF16)
            logs = jnp.where(lane == 2 * h, t0, logs)
            logs = jnp.where(lane == 2 * h + 1, t1, logs)
        logt_ref[:, at] = jnp.log(jnp.transpose(logs)[:8])
        return carry


    def conv_rows_of(i, carry):
        base = pl.multiple_of(i * 64, 64)
        total = jnp.zeros((64, 128), F32)
        for k in range(4):
            out = jnp.zeros((64, 128), F32)
            for j in range(31):
                out = out + taps[pl.ds(j, 1), pl.ds(k * 128, 128)] * gpad[k, pl.ds(base + (j + 2), 64)]
            out = out.astype(BF16).astype(F32)
            conv[pl.ds(base, 64), pl.ds(k * 128, 128)] = out
            total = total + out * out
        squares[pl.ds(base, 64)] = total
        return carry

    sq = pltpu.make_async_remote_copy(
        src_ref=squares, dst_ref=sq_in, send_sem=side_send.at[1], recv_sem=side_recv.at[1],
        device_id={"tp": 1 - core}, device_id_type=MESH,
    )

    def act_rows(i, carry):
        at = pl.ds(pl.multiple_of(i * 128, 128), 128)
        total = jnp.sum(squares[at] + sq_in[at], axis=-1, keepdims=True)
        gain = cgain_ref[pl.ds(pl.multiple_of(core * 512, 512), 512)].astype(F32).reshape(1, 512)
        x = conv[at] * lax.rsqrt(total / CONV + EPS) * gain
        both[at, pl.ds(512, 512)] = (x * jax.nn.sigmoid(x)).astype(BF16)
        return carry

    def out_copy(n):
        return pltpu.make_async_remote_copy(
            src_ref=outbox.at[n], dst_ref=inbox.at[n], send_sem=out_send.at[n], recv_sem=out_recv.at[n],
            device_id={"tp": 1 - core}, device_id_type=MESH,
        )

    theirs = pl.ds(pl.multiple_of((1 - core) * 256, 256), 256)
    ours = pl.ds(pl.multiple_of(core * 256, 256), 256)

    def out_columns(n):
        return jnp.concatenate([wo[8 * n + k] for k in range(8)], axis=1)

    loads[3].wait()
    loads[4].wait()
    step0(WG)
    loads[2].wait()
    step0(WQ)
    loads[0].wait()
    loads[1].wait()
    step0(WKV)
    step1(WG)
    step1(WKV)
    step2(WG)
    step2(WKV)
    step1(WQ)
    step3(WG)
    step3(WKV)
    loads[5].wait()
    lax.fori_loop(0, rows // 64, norm_rows, 0)
    taps[...] = taps_ref[...].astype(F32)
    step2(WQ)
    step4(WKV)
    for c in range(2):
        part = dot(normed[pl.ds(c * half, half)], wkv[...])
        keys_t = jnp.transpose(part[:, :128]).astype(BF16)
        kv[me * 2 + c, pl.ds(0, 128)] = keys_t[:, :128]
        kv[me * 2 + c, pl.ds(128, 128)] = keys_t[:, 128:]
        kv[me * 2 + c, pl.ds(256, 256)] = part[:, 128:].astype(BF16)
    step4(WG)
    planes_start()
    step3(WQ)
    step0(KV)
    step4(WQ)
    for c in range(2):
        at = pl.ds(c * half, half)
        q[at] = dot(normed[at], wq[...]).astype(BF16)
    for c in range(2):
        attend_own(c)
    step1(KV)
    attend_group(0, 2, straight)
    planes_forward(0)
    planes_forward(1)
    loads[7].wait()
    step0(WOB)
    loads[6].wait()
    step0(WOA)
    attend_group(2, 2, straight)
    step2(KV)
    attend_group(0, 2, corner)
    attend_group(2, 2, corner)
    step1(WOA)
    step1(WOB)
    planes_forward(2)
    planes_forward(3)
    attend_group(0, 2, opposite)
    step3(KV)
    attend_group(0, 2, knight)
    for b in range(4):
        for w in range(2):
            plane_message(b, w, True, True).wait_recv()
    step2(WOA)
    gate_rows()
    for k in range(4):
        rim_box[0, k] = gpad[k, pl.ds(rows, 32)].astype(BF16)
    rim.start()
    step2(WOB)
    attend_group(2, 2, knight)
    rim.wait_recv()
    inside = jnp.where(me > 0, 1.0, 0.0)
    for k in range(4):
        gpad[k, pl.ds(0, 32)] = rim_box[1, k].astype(F32) * inside

    lax.fori_loop(0, rows // 64, conv_rows_of, 0)
    sq.start()
    step4(KV)
    step3(WOB)
    step3(WOA)
    attend_group(0, 1, lambda i: (2, 2))
    lax.fori_loop(0, rows // 256, finish_rows, 0)
    sq.wait_recv()
    step4(WOB)
    lax.fori_loop(0, rows // 128, act_rows, 0)
    step4(WOA)
    for n in range(2):
        outbox[n] = dot(both[theirs], out_columns(n)).astype(BF16)
        out_copy(n).start()
    for n in range(2):
        part = dot(both[ours], out_columns(n))
        out_copy(n).wait_recv()
        mixed_ref[:, pl.ds(n * 1024, 1024)] = (part + inbox[n].astype(F32)).astype(BF16)

    for job in range(6):
        for c, w in BOTH:
            for kind in KINDS:
                message(job, c, w, kind).wait_send()
    for b in range(4):
        for w in range(2):
            plane_message(b, w, False).wait_send()
            plane_message(b, w, True).wait_send()
    rim.wait_send()
    sq.wait_send()

    for n in range(2):
        out_copy(n).wait_send()


def body(
    tokens, norm_gain, w_query, w_key, w_value, w_glu_value, w_glu_gate, conv_taps, convolution_norm_gain, head_gain, lam, w_out,
):
    rows = tokens.shape[0]
    d = tokens.shape[1]
    vmem = pl.BlockSpec(memory_space=pltpu.VMEM)
    smem = pl.BlockSpec(memory_space=pltpu.SMEM)
    dma = pltpu.SemaphoreType.DMA
    mixed, logs = pl.pallas_call(
        kernel,
        out_shape=(jax.ShapeDtypeStruct((rows // 2, d), BF16), jax.ShapeDtypeStruct((8, rows), F32)),
        in_specs=[ANY, vmem, ANY, ANY, ANY, ANY, ANY, vmem, vmem, vmem, smem, ANY],
        out_specs=(vmem, vmem),
        scratch_shapes=[
            pltpu.VMEM((rows, d), BF16),
            pltpu.VMEM((rows, d), BF16),
            pltpu.VMEM((d, 256), BF16),
            pltpu.VMEM((d, 512), BF16),
            pltpu.VMEM((4, 2, d, 128), BF16),
            pltpu.VMEM((RING, 1024, 128), BF16),
            pltpu.VMEM((2 * RING, 512, 128), BF16),
            pltpu.VMEM((rows, 512), BF16),
            pltpu.VMEM((8, rows, 128), F32),
            pltpu.VMEM((8, rows, 128), F32),
            pltpu.VMEM((4, rows + 32, 128), F32),
            pltpu.VMEM((rows, 512), F32),
            pltpu.VMEM((rows, 128), F32),
            pltpu.VMEM((rows, 1024), BF16),
            pltpu.VMEM((2, 256, 1024), BF16),
            pltpu.VMEM((2, 256, 1024), BF16),
            pltpu.VMEM((2, 4, 32, 128), BF16),
            pltpu.VMEM((rows, 128), F32),
            pltpu.VMEM((31, 512), F32),
            dma((8,)),
            dma((6, 2, 2, len(KINDS))),
            dma((6, 2, 2, len(KINDS))),
            dma((16,)),
            dma((16,)),
            dma((2,)),
            dma((2,)),
            dma((2,)),
            dma((2,)),
        ],
        compiler_params=pltpu.CompilerParams(
            collective_id=0, has_side_effects=True, vmem_limit_bytes=60 * 1024 * 1024
        ),
    )(
        tokens, norm_gain, w_query, w_key, w_value, w_glu_value, w_glu_gate,
        conv_taps, convolution_norm_gain, head_gain.reshape(1, -1), lam, w_out,
    )
    return mixed, logs.T


def solution(mesh):
    return jax.shard_map(
        body,
        mesh=mesh,
        in_specs=(
            P(("fs", "sp"), None),
            P(),
            P("sp", "tp"),
            P("sp", "tp"),
            P("sp", "tp"),
            P("sp", "tp"),
            P("sp", "tp"),
            P(None, "tp"),
            P(),
            P(),
            P("tp"),
            P(None, "sp"),
        ),
        out_specs=(P(("fs", "sp", "tp"), None), P(("fs", "sp"), "tp")),
        check_vma=False,
    )
```
